32 devices in a mesh: row: 4 (over z), col: 8 (over y, x, core).
Axes of the slice: x: 2, y: 2, z: 4, core: 2. Of those that a mesh axis runs over, the one named last changes fastest.
Arguments:
- tokens: bfloat16 [32, 144, 2048], P('row', 'col'), may hold values from -6 to 6
- norm_gain: bfloat16 [2048], replicated, may hold values from 0.099609375 to 1.8984375
- w_in: bfloat16 [2048, 1152], replicated, may hold values from -0.125 to 0.125
- w_out: bfloat16 [1152, 2048], replicated, may hold values from -0.1875 to 0.1875
Outputs:
- mixed: bfloat16 [144, 32, 2048], P('row', 'col')
The draws below stay inside these ranges and needn't reach their ends.
All inputs are finite; a program needn't handle non-finite values.
Results may differ from the reference program's by a relative error of at most 0.013.
Values may be sent and summed in bfloat16 or wider, within the bound.
No kernel may reach another device: no remote copies, remote signals or barrier semaphores. Data moves between devices by JAX's collectives and lax.ppermute only.
A program may use at most 64 MiB of HBM per device.

```python
import jax
import jax.numpy as jnp
from jax import lax

D = 2048
GROUP = 128
F = 1152
LEN_A = 32
LEN_B = 144
N_COL = 8


def level_of(stream_key, dims, cuts, low, high):
    level = 1.0
    for axis_at, parts in cuts:
        draws = jax.random.uniform(jax.random.fold_in(jax.random.fold_in(stream_key, 6), axis_at), (parts,), jnp.float32, low / len(cuts), high / len(cuts))
        level = level * jnp.repeat(jnp.exp(draws), dims[axis_at] // parts).reshape((-1,) + (1,) * (len(dims) - 1 - axis_at))
    return level


def gaussian(stream_key, dims, scale, bound, cuts=(), kind=jnp.bfloat16):
    array = scale * jax.random.normal(stream_key, dims, jnp.float32)
    if cuts:
        array = array * level_of(stream_key, dims, cuts, -0.22, 0.18)
    return jnp.clip(array, -bound, bound).astype(kind)


def setup_inputs(seed: int = 0) -> dict:
    arg_keys = jax.random.split(jax.random.key(seed), 5)
    tokens = gaussian(arg_keys[0], (LEN_A, LEN_B, D), 1.0, 6.0, ((0, 4), (1, 8)))
    norm_gain = jnp.clip(1.0 + 0.18 * jax.random.normal(arg_keys[1], (D,), jnp.float32), 0.099609375, 1.8984375).astype(jnp.bfloat16)
    w_in = gaussian(arg_keys[2], (D, F), D ** -0.5, 0.125)
    w_out = gaussian(arg_keys[3], (F, D), F ** -0.5, 0.1875)
    return dict(tokens=tokens, norm_gain=norm_gain, w_in=w_in, w_out=w_out)


norm_eps = 1e-06

def folded_order(length_first, devices):
    block = length_first // devices
    half_block = block // 2
    series = jnp.arange(length_first, dtype=jnp.int32)
    device = series // block
    inner = series % block
    lower = device * half_block + inner
    upper = length_first - device * half_block - (inner - half_block)
    upper = jnp.where((device == 0) & (inner == half_block), length_first // 2, upper)
    return (jnp.where(inner < half_block, lower, upper) % length_first).astype(jnp.int32)

def reference(tokens, norm_gain, w_in, w_out):
    length_first, length_second, features = tokens.shape
    positions = length_first * length_second
    floats = tokens.astype(jnp.float32).reshape(positions, features)
    normed = (floats * lax.rsqrt(lax.optimization_barrier(jnp.mean(floats * floats, axis=-1, keepdims=True)) + norm_eps) * norm_gain.astype(jnp.float32)).astype(jnp.bfloat16)
    mapped = jnp.dot(normed, w_in, preferred_element_type=jnp.float32).astype(jnp.bfloat16)
    channels = mapped.shape[1]
    grouped = mapped.astype(jnp.float32).reshape(positions, channels // GROUP, GROUP).transpose(1, 0, 2)

    def one_group(block):
        return jnp.fft.fft2(block, norm='ortho').real.astype(jnp.float32)
    spectrum = lax.map(one_group, grouped).transpose(1, 0, 2).reshape(positions, channels)
    spectrum = spectrum.astype(jnp.bfloat16)
    mixed = jnp.dot(spectrum, w_out, preferred_element_type=jnp.float32).astype(jnp.bfloat16)
    mixed = mixed.reshape(length_second, length_first, features)
    return jnp.take(mixed, folded_order(length_first, N_COL), axis=1)
```

```python
import functools
import math

import jax
import jax.numpy as jnp
import numpy as np
from jax import lax
from jax.experimental import pallas as pl
from jax.experimental.pallas import tpu as pltpu
from jax.sharding import PartitionSpec as P

GROUP = 128


norm_eps = 1e-06
highest = lax.Precision.HIGHEST


def tables(length):
    series = jnp.arange(length, dtype=jnp.int32)
    product = series[:, None] * series[None, :] % length
    angles = product.astype(jnp.float32) * (2.0 * math.pi / length)
    return (jnp.cos(angles), jnp.sin(angles))


def folded_order(length_first, devices):
    block = length_first // devices
    half_block = block // 2
    series = jnp.arange(length_first, dtype=jnp.int32)
    device = series // block
    inner = series % block
    lower = device * half_block + inner
    upper = length_first - device * half_block - (inner - half_block)
    upper = jnp.where((device == 0) & (inner == half_block), length_first // 2, upper)
    return jnp.where(inner < half_block, lower, upper) % length_first


def to_channels(values, row_count):
    rows_first, rows_second, channels = values.shape
    width = channels // row_count
    parted = values.reshape(rows_first, rows_second, row_count, width).transpose(2, 0, 1, 3)
    return parted.reshape(row_count * rows_first, rows_second * width)


def product(table, values):
    return jnp.dot(table, values, precision=highest)


def middle(real_part, imag_part, width):
    length_first = real_part.shape[0]
    rows_second = real_part.shape[1] // width
    col_count = lax.axis_size("col")
    length_second = rows_second * col_count
    positions = length_first * length_second
    frequency = folded_order(length_first, col_count)
    series = jnp.arange(length_first, dtype=jnp.int32)
    first_angle = (frequency[:, None] * series[None, :] % length_first).astype(jnp.float32)
    first_angle = first_angle * (2.0 * math.pi / length_first)
    first_cos = jnp.cos(first_angle)
    first_sin = jnp.sin(first_angle)
    first_real = product(first_cos, real_part)
    first_imag = -product(first_sin, real_part)
    first_real = first_real + product(first_sin, imag_part)
    first_imag = first_imag + product(first_cos, imag_part)
    first_real = first_real.reshape(length_first, rows_second, width)
    first_imag = first_imag.reshape(length_first, rows_second, width)
    second_index = lax.axis_index("col") * rows_second + jnp.arange(rows_second, dtype=jnp.int32)
    twiddle_angle = (frequency[:, None] * second_index[None, :] % positions).astype(jnp.float32)
    twiddle_angle = twiddle_angle * (2.0 * math.pi / positions)
    twiddle_cos = jnp.cos(twiddle_angle)[:, :, None]
    twiddle_sin = jnp.sin(twiddle_angle)[:, :, None]
    turned_real = first_real * twiddle_cos + first_imag * twiddle_sin
    turned_imag = first_imag * twiddle_cos - first_real * twiddle_sin
    turned = jnp.stack([turned_real, turned_imag]).transpose(0, 2, 1, 3)
    turned = turned.reshape(2, rows_second, length_first * width)
    exchanged = lax.all_to_all(
        turned.astype(jnp.bfloat16), "col", split_axis=2, concat_axis=1, tiled=True
    ).astype(turned.dtype)
    second_cos, second_sin = tables(length_second)
    block = length_first // col_count
    out_shape = (length_second, block, width)
    out_real = (product(second_cos, exchanged[0]) + product(second_sin, exchanged[1])).reshape(
        out_shape
    )
    return out_real


def general(tokens, norm_gain, w_in, w_out):
    rows_first, rows_second, features = tokens.shape
    row_count = lax.axis_size("row")
    length_first = rows_first * row_count
    length_second = rows_second * lax.axis_size("col")
    channels = w_in.shape[1]
    width = channels // row_count
    groups = channels // GROUP
    scaling = 1.0 / math.sqrt(length_first * length_second * GROUP)
    floats = tokens.astype(jnp.float32)
    normed = (
        floats
        * lax.rsqrt(jnp.mean(floats * floats, axis=-1, keepdims=True) + norm_eps)
        * norm_gain.astype(jnp.float32)
    ).astype(jnp.bfloat16)
    mapped = jnp.dot(normed.reshape(-1, features), w_in, preferred_element_type=jnp.float32)
    mapped = mapped.astype(jnp.bfloat16).reshape(rows_first, rows_second, channels)
    channel_cos, channel_sin = tables(GROUP)
    grouped = mapped.astype(jnp.float32).reshape(rows_first, rows_second, groups, GROUP)
    spec_real = jnp.einsum("abgj,jm->abgm", grouped, channel_cos, precision=highest)
    spec_imag = -jnp.einsum("abgj,jm->abgm", grouped, channel_sin, precision=highest)
    stacked = jnp.stack(
        [
            to_channels(spec_real.reshape(rows_first, rows_second, channels), row_count),
            to_channels(spec_imag.reshape(rows_first, rows_second, channels), row_count),
        ]
    )
    arrived = lax.all_to_all(
        stacked.astype(jnp.bfloat16), "row", split_axis=1, concat_axis=1, tiled=True
    ).astype(stacked.dtype)
    result = middle(arrived[0], arrived[1], width)
    spectrum = (result * scaling).astype(jnp.bfloat16)
    returned = lax.all_to_all(spectrum, "row", split_axis=0, concat_axis=2, tiled=True)
    mixed = jnp.dot(returned.reshape(-1, channels), w_out, preferred_element_type=jnp.float32)
    return mixed.astype(jnp.bfloat16).reshape(returned.shape[0], returned.shape[1], features)


LANES = 128
TILE = 8
VMEM = pl.BlockSpec(memory_space=pltpu.VMEM)
ANY = pl.BlockSpec(memory_space=pl.ANY)


class Plan:
    def __init__(self, rows, cols, rows_first, rows_second, features, channels):
        self.rows, self.cols = rows, cols
        self.rows_first, self.rows_second = rows_first, rows_second
        self.features, self.channels = features, channels
        self.length_first = rows_first * rows
        self.length_second = rows_second * cols
        self.positions = self.length_first * self.length_second
        self.groups = channels // GROUP
        self.full = self.groups // rows
        self.sub = GROUP // rows
        self.half = rows_second // 2
        self.quads = -(-self.half // rows)
        self.tiles = self.full * self.half + self.quads
        self.local = rows_first * rows_second
        self.send_rows = self.full * self.local + 2 * self.quads * TILE
        self.pairs = self.length_first // cols // 2
        self.block_b = self.length_second // rows
        self.out_rows = self.block_b * 2 * self.pairs
        self.row_tiles = self.out_rows // TILE
        self.back_quads = -(-self.row_tiles // rows)
        self.back_rows = self.full * self.out_rows + self.back_quads * TILE

    def fits(self):
        return (
            GROUP == LANES
            and self.rows & (self.rows - 1) == 0
            and self.cols & (self.cols - 1) == 0
            and 1 < self.rows <= 8
            and self.cols > 1
            and self.rows_first == TILE
            and self.rows_second % 2 == 0
            and self.channels % GROUP == 0
            and self.groups % self.rows == 1
            and self.full == 2
            and self.length_first == 4 * self.cols
            and self.length_second % self.rows == 0
            and 2 * self.block_b % TILE == 0
            and self.features % 256 == 0
        )


def channel_table():
    j = np.arange(GROUP)[:, None]
    u = np.arange(GROUP)[None, :]
    half = GROUP // 2
    m = np.where(u <= half, u, u - half)
    angle = 2.0 * np.pi * (j * m % GROUP) / GROUP
    return np.where(u <= half, np.cos(angle), np.sin(angle))


def unfold_table():
    half = GROUP // 2
    table = np.zeros((GROUP, GROUP))
    for m in range(GROUP):
        near = m if m <= half else GROUP - m
        table[near, m] = 1.0
        if 0 < near < half:
            table[half + near, m] = -1.0 if m < half else 1.0
    return table


def paired(table):
    zero = np.zeros_like(table)
    return np.block([[table, zero], [zero, table]])


def first_tables(plan):
    a = np.arange(plan.length_first)
    out = np.zeros((plan.cols, plan.half, plan.cols, plan.pairs, 2, 2, 2, plan.length_first))
    for col in range(plan.cols):
        for b9 in range(plan.half):
            for h in range(2):
                b = col * plan.rows_second + h * plan.half + b9
                for c in range(plan.cols):
                    for i in range(plan.pairs):
                        k = c * plan.pairs + i
                        if k == 0:
                            out[col, b9, c, i, h, 0, h] = 1.0
                            out[col, b9, c, i, h, 1, h] = np.where(a % 2 == 0, 1.0, -1.0)
                        else:
                            phase = (a * plan.length_second + b) * k % plan.positions
                            angle = 2.0 * np.pi * phase / plan.positions
                            out[col, b9, c, i, h, 0, h] = np.cos(angle)
                            out[col, b9, c, i, h, 1, h] = -np.sin(angle)
    size = 2 * plan.length_first
    return out.reshape(plan.cols, plan.half, size, size)


def second_tables(plan):
    length = plan.length_second
    b9 = np.arange(plan.half)[:, None, None]
    c = np.arange(plan.cols)[None, :, None]
    h = np.arange(2)[None, None, :]
    b = (c * plan.rows_second + h * plan.half + b9).reshape(-1)
    k = np.arange(length)
    angle = 2.0 * np.pi * (k[:, None] * b[None, :] % length) / length
    cos, sin = np.cos(angle), np.sin(angle)
    cosine = np.stack([cos, sin], axis=-1)
    sine = np.stack([sin, -cos], axis=-1)

    def arrange(plus, minus):
        both = np.stack([plus, minus]).reshape(2, plan.rows, plan.block_b, -1)
        return both.transpose(1, 0, 2, 3).reshape(2 * length, -1)

    usual = np.stack([arrange(cosine, cosine[::-1]), arrange(sine, -sine[::-1])])
    turn = 2.0 * np.pi * ((plan.length_first // 2) * b % plan.positions) / plan.positions
    late = angle + turn[None, :]
    zero = np.zeros_like(cos)
    first = np.stack(
        [
            arrange(np.stack([cos, zero], -1), np.stack([zero, np.cos(late)], -1)),
            arrange(np.stack([sin, zero], -1), np.stack([zero, np.sin(late)], -1)),
        ]
    )
    return usual, first


def order_table(plan):
    table = np.zeros((plan.out_rows, plan.out_rows))
    for i in range(plan.pairs):
        for neg in range(2):
            for k in range(plan.block_b):
                row = (k * 2 + neg) * plan.pairs + i
                table[row, (i * 2 + neg) * plan.block_b + k] = 1.0
    return table


def dot(left, right):
    return jnp.dot(left, right, preferred_element_type=jnp.float32)


def lane_index(shape):
    return lax.broadcasted_iota(jnp.int32, shape, 1)


def turn_lanes(value, amount):
    amount = amount % LANES
    return value if amount == 0 else pltpu.roll(value, amount, 1)


def by_lane(pieces, sub):
    out = pieces[0]
    lane = lane_index(out.shape)
    for n in range(1, len(pieces)):
        out = jnp.where(lane >= n * sub, pieces[n], out)
    return out


def head_kernel(plan, x_hbm, gain_ref, w_hbm, table_ref, out_ref, x_ref, normed_ref, w_ref, x_sem, w_sems):
    chunks = plan.full * plan.rows // 2
    wide = 2 * GROUP
    spans = [(n * wide, wide) for n in range(chunks)] + [(chunks * wide, GROUP)]
    x_copy = pltpu.make_async_copy(x_hbm, x_ref, x_sem)
    x_copy.start()
    copies = []
    for n, (start, size) in enumerate(spans):
        copy = pltpu.make_async_copy(
            w_hbm.at[:, pl.ds(start, size)], w_ref.at[:, pl.ds(start, size)], w_sems.at[n]
        )
        copy.start()
        copies.append(copy)
    x_copy.wait()
    gain = gain_ref[...].astype(jnp.float32)
    step = 48 if plan.local % 48 == 0 else TILE
    for start in range(0, plan.local, step):
        floats = x_ref[start : start + step, :].astype(jnp.float32)
        scale = lax.rsqrt(jnp.mean(floats * floats, axis=-1, keepdims=True) + norm_eps)
        normed_ref[start : start + step, :] = (floats * scale * gain).astype(jnp.bfloat16)
    sub = plan.sub
    for n, (start, size) in enumerate(spans):
        copies[n].wait()
        mapped = dot(normed_ref[...], w_ref[:, start : start + size]).astype(jnp.bfloat16)
        values = dot(mapped, table_ref[:size, :size])
        if size == wide:
            for f in range(2):
                out_ref[n, f * plan.local : (f + 1) * plan.local, :] = values[
                    :, f * GROUP : (f + 1) * GROUP
                ].astype(jnp.bfloat16)
            continue
        turned = [turn_lanes(values, sub * t) for t in range(plan.rows)]
        base = plan.full * plan.local
        for dest in range(plan.rows):
            for h in range(2):
                for quad in range(plan.quads):
                    pieces = []
                    for inner in range(plan.rows):
                        b9 = quad * plan.rows + inner
                        if b9 < plan.half:
                            row = (h * plan.half + b9) * TILE
                            pieces.append(turned[(inner - dest) % plan.rows][row : row + TILE, :])
                    at = base + (h * plan.quads + quad) * TILE
                    out_ref[dest, at : at + TILE, :] = by_lane(pieces, sub).astype(jnp.bfloat16)


def first_kernel(plan, *refs):
    slabs, (table_ref, out_ref, held_ref) = refs[: plan.rows], refs[plan.rows :]
    row = lax.axis_index("row")
    for s in range(plan.rows):
        held_ref[row ^ s] = slabs[s][...]
    for b9 in range(plan.half):
        quad, inner = divmod(b9, plan.rows)
        columns = []
        for f in range(plan.full):
            parts = []
            for h in range(2):
                at = f * plan.local + (h * plan.half + b9) * TILE
                parts += [held_ref[r, at : at + TILE, :] for r in range(plan.rows)]
            columns.append(jnp.concatenate(parts, axis=0))
        parts = []
        for h in range(2):
            at = plan.full * plan.local + (h * plan.quads + quad) * TILE
            parts += [held_ref[r, at : at + TILE, :] for r in range(plan.rows)]
        columns.append(jnp.concatenate(parts, axis=0))
        result = dot(table_ref[b9], jnp.concatenate(columns, axis=1))
        for f in range(plan.full):
            at = (f * plan.half + b9) * TILE
            piece = result[:, f * LANES : (f + 1) * LANES].astype(jnp.bfloat16)
            for c in range(plan.cols):
                out_ref[c, at : at + TILE, :] = piece[c * TILE : (c + 1) * TILE, :]
        tail = result[:, plan.full * LANES :]
        packed = tail if inner == 0 else jnp.where(lane_index(tail.shape) >= inner * plan.sub, tail, packed)
        if inner == plan.rows - 1 or b9 == plan.half - 1:
            at = (plan.full * plan.half + quad) * TILE
            piece = packed.astype(jnp.bfloat16)
            for c in range(plan.cols):
                out_ref[c, at : at + TILE, :] = piece[c * TILE : (c + 1) * TILE, :]


def second_kernel(plan, scaling, *refs):
    slabs = refs[: plan.cols]
    usual_ref, first_ref, out_ref, held_ref, rhs_ref = refs[plan.cols :]
    row, col = lax.axis_index("row"), lax.axis_index("col")
    for s in range(plan.cols):
        held_ref[col ^ s] = slabs[s][...]
    sub, quarter = plan.sub, TILE // 2
    low = lax.broadcasted_iota(jnp.int32, (TILE, LANES), 0) < quarter
    for b9 in range(plan.half):
        quad, inner = divmod(b9, plan.rows)
        places = [(f * plan.half + b9) * TILE for f in range(plan.full)]
        places.append((plan.full * plan.half + quad) * TILE)
        for p in range(plan.cols // 2):
            at = b9 * (plan.cols // 2) * TILE + p * TILE
            for n, place in enumerate(places):
                even = held_ref[2 * p, place : place + TILE, :].astype(jnp.float32)
                odd = held_ref[2 * p + 1, place : place + TILE, :].astype(jnp.float32)
                both = [
                    jnp.where(low, even, pltpu.roll(odd, quarter, 0)),
                    jnp.where(low, pltpu.roll(even, quarter, 0), odd),
                ]
                for i in range(plan.pairs):
                    value = both[i]
                    if n == plan.full:
                        value = turn_lanes(value, -inner * sub)
                    rhs_ref[i, at : at + TILE, n * LANES : (n + 1) * LANES] = value.astype(jnp.bfloat16)
    wide = (plan.full + 1) * LANES
    lane = lane_index((1, wide))
    last = lane >= plan.full * LANES
    place = jnp.where(last, lane - plan.full * LANES + row * sub, lane & (LANES - 1))
    is_sine = place > GROUP // 2
    span = 2 * plan.block_b
    kept = {}
    for i in range(plan.pairs):
        table = first_ref if i == 0 else usual_ref
        values = rhs_ref[i]
        for r in range(plan.rows):
            cosine = dot(table[0, r * span : (r + 1) * span, :], values)
            sine = dot(table[1, r * span : (r + 1) * span, :], values)
            merged = jnp.where(is_sine, sine, cosine) * scaling
            for f in range(plan.full):
                at = f * plan.out_rows + i * span
                out_ref[r, at : at + span, :] = merged[:, f * LANES : (f + 1) * LANES].astype(jnp.bfloat16)
            tail = merged[:, plan.full * LANES :]
            for t in range(span // TILE):
                whole, inner = divmod(i * (span // TILE) + t, plan.rows)
                at = plan.full * plan.out_rows + whole * TILE
                piece = turn_lanes(tail[t * TILE : (t + 1) * TILE, :], inner * sub)
                if inner:
                    piece = jnp.where(lane_index(piece.shape) >= inner * sub, piece, kept[r])
                kept[r] = piece
                if inner == plan.rows - 1 or (i == plan.pairs - 1 and t == span // TILE - 1):
                    out_ref[r, at : at + TILE, :] = piece.astype(jnp.bfloat16)


def tail_kernel(plan, *refs):
    slabs = refs[: plan.rows]
    unfold_ref, order_ref, w_ref, out_ref, held_ref, spectrum_ref = refs[plan.rows :]
    row = lax.axis_index("row")
    for s in range(plan.rows):
        held_ref[row ^ s] = slabs[s][...]
    order = order_ref[...]
    unfold = unfold_ref[...]
    for q in range(plan.rows):
        pair = [held_ref[q, f * plan.out_rows : (f + 1) * plan.out_rows, :] for f in range(plan.full)]
        ordered = dot(order, jnp.concatenate(pair, axis=1)).astype(jnp.bfloat16)
        spectrum_ref[:, q * 2 * GROUP : (q + 1) * 2 * GROUP] = dot(ordered, unfold).astype(jnp.bfloat16)
    base = plan.full * plan.out_rows
    packed = [held_ref[q, base:, :].astype(jnp.float32) for q in range(plan.rows)]
    turned = [[turn_lanes(value, plan.sub * t) for t in range(plan.rows)] for value in packed]
    pieces = []
    for t in range(plan.row_tiles):
        whole, inner = divmod(t, plan.rows)
        rows = slice(whole * TILE, (whole + 1) * TILE)
        pieces.append(
            by_lane([turned[q][(q - inner) % plan.rows][rows, :] for q in range(plan.rows)], plan.sub)
        )
    last = jnp.concatenate(pieces, axis=0).astype(jnp.bfloat16)
    ordered = dot(order, last).astype(jnp.bfloat16)
    spectrum_ref[:, plan.rows * 2 * GROUP :] = dot(ordered, unfold[:GROUP, :GROUP]).astype(jnp.bfloat16)
    wide = 256
    group = 2 * plan.pairs
    for n in range(plan.features // wide):
        columns = slice(n * wide, (n + 1) * wide)
        result = dot(spectrum_ref[...], w_ref[:, columns]).astype(jnp.bfloat16)
        for k in range(plan.block_b):
            out_ref[k, :, columns] = result[k * group : (k + 1) * group, :]


def estimate(flops, moved):
    return pl.CostEstimate(flops=flops, bytes_accessed=moved, transcendentals=0)


def limit(mebibytes):
    return pltpu.CompilerParams(vmem_limit_bytes=mebibytes * 2**20)


def exchange(values, axis, size):
    here = lax.axis_index(axis)
    out = [lax.dynamic_index_in_dim(values, here, 0, keepdims=False)]
    for s in range(1, size):
        slab = lax.dynamic_index_in_dim(values, here ^ s, 0, keepdims=False)
        out.append(lax.ppermute(slab, axis, [(n, n ^ s) for n in range(size)]))
    return out


def packed(plan, tokens, norm_gain, w_in, w_out):
    half_type = jnp.bfloat16
    scaling = 1.0 / math.sqrt(plan.positions * GROUP)
    col = lax.axis_index("col")
    local, features, channels = plan.local, plan.features, plan.channels
    x = tokens.transpose(1, 0, 2).reshape(local, features)
    channel = jnp.asarray(paired(channel_table()), half_type)
    spans = plan.groups // 2 + 1
    sent = pl.pallas_call(
        functools.partial(head_kernel, plan),
        out_shape=jax.ShapeDtypeStruct((plan.rows, plan.send_rows, LANES), half_type),
        in_specs=[ANY, VMEM, ANY, VMEM],
        out_specs=VMEM,
        scratch_shapes=[
            pltpu.VMEM((local, features), half_type),
            pltpu.VMEM((local, features), half_type),
            pltpu.VMEM((features, channels), half_type),
            pltpu.SemaphoreType.DMA,
            pltpu.SemaphoreType.DMA((spans,)),
        ],
        compiler_params=limit(16),
        cost_estimate=estimate(2 * local * features * channels, 2 * features * channels),
        name="head",
    )(x, norm_gain.reshape(1, features), w_in, channel)
    slabs = exchange(sent, "row", plan.rows)
    first = lax.dynamic_index_in_dim(jnp.asarray(first_tables(plan), half_type), col, 0, keepdims=False)
    turned = pl.pallas_call(
        functools.partial(first_kernel, plan),
        out_shape=jax.ShapeDtypeStruct((plan.cols, plan.tiles * TILE, LANES), half_type),
        in_specs=[VMEM] * (plan.rows + 1),
        out_specs=VMEM,
        scratch_shapes=[pltpu.VMEM((plan.rows, plan.send_rows, LANES), half_type)],
        compiler_params=limit(8),
        cost_estimate=estimate(10**8, 10**6),
        name="first",
    )(*slabs, first)
    slabs = exchange(turned, "col", plan.cols)
    usual, special = (jnp.asarray(table, half_type) for table in second_tables(plan))
    leading = jnp.where(col == 0, special, usual)
    depth = plan.half * plan.cols * 4
    back = pl.pallas_call(
        functools.partial(second_kernel, plan, scaling),
        out_shape=jax.ShapeDtypeStruct((plan.rows, plan.back_rows, LANES), half_type),
        in_specs=[VMEM] * (plan.cols + 2),
        out_specs=VMEM,
        scratch_shapes=[
            pltpu.VMEM((plan.cols, plan.tiles * TILE, LANES), half_type),
            pltpu.VMEM((plan.pairs, depth, (plan.full + 1) * LANES), half_type),
        ],
        compiler_params=limit(12),
        cost_estimate=estimate(3 * 10**8, 10**6),
        name="second",
    )(*slabs, usual, leading)
    slabs = exchange(back, "row", plan.rows)
    return pl.pallas_call(
        functools.partial(tail_kernel, plan),
        out_shape=jax.ShapeDtypeStruct((plan.block_b, 2 * plan.pairs, features), half_type),
        in_specs=[VMEM] * (plan.rows + 3),
        out_specs=VMEM,
        scratch_shapes=[
            pltpu.VMEM((plan.rows, plan.back_rows, LANES), half_type),
            pltpu.VMEM((plan.out_rows, channels), half_type),
        ],
        compiler_params=limit(12),
        cost_estimate=estimate(2 * local * features * channels, 2 * features * channels),
        name="tail",
    )(*slabs, jnp.asarray(paired(unfold_table()), half_type), jnp.asarray(order_table(plan), half_type), w_out)


def shards(tokens, norm_gain, w_in, w_out):
    rows_first, rows_second, features = tokens.shape
    plan = Plan(
        lax.axis_size("row"), lax.axis_size("col"), rows_first, rows_second, features, w_in.shape[1]
    )
    if plan.fits():
        return packed(plan, tokens, norm_gain, w_in, w_out)
    return general(tokens, norm_gain, w_in, w_out)


def solution(mesh):
    in_specs = (P("row", "col", None), P(), P(), P())
    out_specs = P("row", "col", None)
    return jax.shard_map(shards, mesh=mesh, in_specs=in_specs, out_specs=out_specs, check_vma=False)
```

```python
import functools
import math

import jax
import jax.numpy as jnp
import numpy as np
from jax import lax
from jax.experimental import pallas as pl
from jax.experimental.pallas import tpu as pltpu
from jax.sharding import PartitionSpec as P

GROUP = 128


norm_eps = 1e-06
highest = lax.Precision.HIGHEST


def tables(length):
    series = jnp.arange(length, dtype=jnp.int32)
    product = series[:, None] * series[None, :] % length
    angles = product.astype(jnp.float32) * (2.0 * math.pi / length)
    return (jnp.cos(angles), jnp.sin(angles))


def folded_order(length_first, devices):
    block = length_first // devices
    half_block = block // 2
    series = jnp.arange(length_first, dtype=jnp.int32)
    device = series // block
    inner = series % block
    lower = device * half_block + inner
    upper = length_first - device * half_block - (inner - half_block)
    upper = jnp.where((device == 0) & (inner == half_block), length_first // 2, upper)
    return jnp.where(inner < half_block, lower, upper) % length_first


def to_channels(values, row_count):
    rows_first, rows_second, channels = values.shape
    width = channels // row_count
    parted = values.reshape(rows_first, rows_second, row_count, width).transpose(2, 0, 1, 3)
    return parted.reshape(row_count * rows_first, rows_second * width)


def product(table, values):
    return jnp.dot(table, values, precision=highest)


def middle(real_part, imag_part, width):
    length_first = real_part.shape[0]
    rows_second = real_part.shape[1] // width
    col_count = lax.axis_size("col")
    length_second = rows_second * col_count
    positions = length_first * length_second
    frequency = folded_order(length_first, col_count)
    series = jnp.arange(length_first, dtype=jnp.int32)
    first_angle = (frequency[:, None] * series[None, :] % length_first).astype(jnp.float32)
    first_angle = first_angle * (2.0 * math.pi / length_first)
    first_cos = jnp.cos(first_angle)
    first_sin = jnp.sin(first_angle)
    first_real = product(first_cos, real_part)
    first_imag = -product(first_sin, real_part)
    first_real = first_real + product(first_sin, imag_part)
    first_imag = first_imag + product(first_cos, imag_part)
    first_real = first_real.reshape(length_first, rows_second, width)
    first_imag = first_imag.reshape(length_first, rows_second, width)
    second_index = lax.axis_index("col") * rows_second + jnp.arange(rows_second, dtype=jnp.int32)
    twiddle_angle = (frequency[:, None] * second_index[None, :] % positions).astype(jnp.float32)
    twiddle_angle = twiddle_angle * (2.0 * math.pi / positions)
    twiddle_cos = jnp.cos(twiddle_angle)[:, :, None]
    twiddle_sin = jnp.sin(twiddle_angle)[:, :, None]
    turned_real = first_real * twiddle_cos + first_imag * twiddle_sin
    turned_imag = first_imag * twiddle_cos - first_real * twiddle_sin
    turned = jnp.stack([turned_real, turned_imag]).transpose(0, 2, 1, 3)
    turned = turned.reshape(2, rows_second, length_first * width)
    exchanged = lax.all_to_all(
        turned.astype(jnp.bfloat16), "col", split_axis=2, concat_axis=1, tiled=True
    ).astype(turned.dtype)
    second_cos, second_sin = tables(length_second)
    block = length_first // col_count
    out_shape = (length_second, block, width)
    out_real = (product(second_cos, exchanged[0]) + product(second_sin, exchanged[1])).reshape(
        out_shape
    )
    return out_real


def general(tokens, norm_gain, w_in, w_out):
    rows_first, rows_second, features = tokens.shape
    row_count = lax.axis_size("row")
    length_first = rows_first * row_count
    length_second = rows_second * lax.axis_size("col")
    channels = w_in.shape[1]
    width = channels // row_count
    groups = channels // GROUP
    scaling = 1.0 / math.sqrt(length_first * length_second * GROUP)
    floats = tokens.astype(jnp.float32)
    normed = (
        floats
        * lax.rsqrt(jnp.mean(floats * floats, axis=-1, keepdims=True) + norm_eps)
        * norm_gain.astype(jnp.float32)
    ).astype(jnp.bfloat16)
    mapped = jnp.dot(normed.reshape(-1, features), w_in, preferred_element_type=jnp.float32)
    mapped = mapped.astype(jnp.bfloat16).reshape(rows_first, rows_second, channels)
    channel_cos, channel_sin = tables(GROUP)
    grouped = mapped.astype(jnp.float32).reshape(rows_first, rows_second, groups, GROUP)
    spec_real = jnp.einsum("abgj,jm->abgm", grouped, channel_cos, precision=highest)
    spec_imag = -jnp.einsum("abgj,jm->abgm", grouped, channel_sin, precision=highest)
    stacked = jnp.stack(
        [
            to_channels(spec_real.reshape(rows_first, rows_second, channels), row_count),
            to_channels(spec_imag.reshape(rows_first, rows_second, channels), row_count),
        ]
    )
    arrived = lax.all_to_all(
        stacked.astype(jnp.bfloat16), "row", split_axis=1, concat_axis=1, tiled=True
    ).astype(stacked.dtype)
    result = middle(arrived[0], arrived[1], width)
    spectrum = (result * scaling).astype(jnp.bfloat16)
    returned = lax.all_to_all(spectrum, "row", split_axis=0, concat_axis=2, tiled=True)
    mixed = jnp.dot(returned.reshape(-1, channels), w_out, preferred_element_type=jnp.float32)
    return mixed.astype(jnp.bfloat16).reshape(returned.shape[0], returned.shape[1], features)


LANES = 128
TILE = 8
STEPS = 2
VMEM = pl.BlockSpec(memory_space=pltpu.VMEM)
HBM = pl.BlockSpec(memory_space=pltpu.HBM)


class Plan:
    def __init__(self, rows, cols, rows_first, rows_second, features, channels):
        self.rows, self.cols = rows, cols
        self.rows_first, self.rows_second = rows_first, rows_second
        self.features, self.channels = features, channels
        self.length_first = rows_first * rows
        self.length_second = rows_second * cols
        self.positions = self.length_first * self.length_second
        self.groups = channels // GROUP
        self.full = self.groups // rows
        self.sub = GROUP // rows
        self.half = rows_second // 2
        self.quads = -(-self.half // rows)
        self.tiles = self.full * self.half + self.quads
        self.local = rows_first * rows_second
        self.half_wide = rows // 2 * self.full * GROUP
        self.send_rows = self.full * self.local + 2 * self.quads * TILE
        self.pairs = self.length_first // cols // 2
        self.block_b = self.length_second // rows
        self.out_rows = self.block_b * 2 * self.pairs
        self.row_tiles = self.out_rows // TILE
        self.back_quads = -(-self.row_tiles // rows)
        self.back_rows = self.full * self.out_rows + self.back_quads * TILE

    def fits(self):
        return (
            GROUP == LANES
            and self.rows & (self.rows - 1) == 0
            and self.cols & (self.cols - 1) == 0
            and 1 < self.rows <= 8
            and self.cols > 1
            and self.rows_first == TILE
            and self.rows_second % 2 == 0
            and self.channels % GROUP == 0
            and self.groups % self.rows == 1
            and self.full == 2
            and self.length_first == 4 * self.cols
            and self.length_second % self.rows == 0
            and 2 * self.block_b % TILE == 0
            and self.features % 256 == 0
        )


def channel_table():
    j = np.arange(GROUP)[:, None]
    u = np.arange(GROUP)[None, :]
    half = GROUP // 2
    m = np.where(u <= half, u, u - half)
    angle = 2.0 * np.pi * (j * m % GROUP) / GROUP
    return np.where(u <= half, np.cos(angle), np.sin(angle))


def unfold_table():
    half = GROUP // 2
    table = np.zeros((GROUP, GROUP))
    for m in range(GROUP):
        near = m if m <= half else GROUP - m
        table[near, m] = 1.0
        if 0 < near < half:
            table[half + near, m] = -1.0 if m < half else 1.0
    return table


def paired(table):
    zero = np.zeros_like(table)
    return np.block([[table, zero], [zero, table]])


def first_tables(plan):
    a = np.arange(plan.length_first)
    out = np.zeros((plan.cols, plan.half, plan.cols, plan.pairs, 2, 2, 2, plan.length_first))
    for col in range(plan.cols):
        for b9 in range(plan.half):
            for h in range(2):
                b = col * plan.rows_second + h * plan.half + b9
                for c in range(plan.cols):
                    for i in range(plan.pairs):
                        k = c * plan.pairs + i
                        if k == 0:
                            out[col, b9, c, i, h, 0, h] = 1.0
                            out[col, b9, c, i, h, 1, h] = np.where(a % 2 == 0, 1.0, -1.0)
                        else:
                            phase = (a * plan.length_second + b) * k % plan.positions
                            angle = 2.0 * np.pi * phase / plan.positions
                            out[col, b9, c, i, h, 0, h] = np.cos(angle)
                            out[col, b9, c, i, h, 1, h] = -np.sin(angle)
    size = 2 * plan.length_first
    return out.reshape(plan.cols, plan.half, size, size)


def second_tables(plan):
    length = plan.length_second
    b9 = np.arange(plan.half)[:, None, None]
    c = np.arange(plan.cols)[None, :, None]
    h = np.arange(2)[None, None, :]
    b = (c * plan.rows_second + h * plan.half + b9).reshape(-1)
    k = np.arange(length)
    angle = 2.0 * np.pi * (k[:, None] * b[None, :] % length) / length
    cos, sin = np.cos(angle), np.sin(angle)
    cosine = np.stack([cos, sin], axis=-1)
    sine = np.stack([sin, -cos], axis=-1)

    def arrange(plus, minus):
        both = np.stack([plus, minus]).reshape(2, plan.rows, plan.block_b, -1)
        return both.transpose(1, 0, 2, 3).reshape(2 * length, -1)

    usual = np.stack([arrange(cosine, cosine[::-1]), arrange(sine, -sine[::-1])])
    turn = 2.0 * np.pi * ((plan.length_first // 2) * b % plan.positions) / plan.positions
    late = angle + turn[None, :]
    zero = np.zeros_like(cos)
    first = np.stack(
        [
            arrange(np.stack([cos, zero], -1), np.stack([zero, np.cos(late)], -1)),
            arrange(np.stack([sin, zero], -1), np.stack([zero, np.sin(late)], -1)),
        ]
    )
    return usual, first


def order_table(plan):
    table = np.zeros((plan.out_rows, plan.out_rows))
    for i in range(plan.pairs):
        for neg in range(2):
            for k in range(plan.block_b):
                row = (k * 2 + neg) * plan.pairs + i
                table[row, (i * 2 + neg) * plan.block_b + k] = 1.0
    return table


def dot(left, right):
    return jnp.dot(left, right, preferred_element_type=jnp.float32)


def lane_index(shape):
    return lax.broadcasted_iota(jnp.int32, shape, 1)


def turn_lanes(value, amount):
    amount = amount % LANES
    return value if amount == 0 else pltpu.roll(value, amount, 1)


def by_lane(pieces, sub):
    out = pieces[0]
    lane = lane_index(out.shape)
    for n in range(1, len(pieces)):
        out = jnp.where(lane >= n * sub, pieces[n], out)
    return out


def far_kernel(
    plan, depth, x_hbm, gain_hbm, w_hbm, table_hbm, out_ref, near_ref, normed_ref, x_ref, gain_ref, table_ref, w_ref, sems, w_sems
):
    wide = plan.half_wide
    other = 1 - lax.axis_index("row") // (plan.rows // 2)
    x_copy = pltpu.make_async_copy(x_hbm, x_ref, sems.at[0])
    gain_copy = pltpu.make_async_copy(gain_hbm, gain_ref, sems.at[1])
    table_copy = pltpu.make_async_copy(table_hbm, table_ref, sems.at[2])
    x_copy.start()
    gain_copy.start()
    steps = plan.features // depth
    copies = []
    for n in range(steps):
        rows = pl.ds(n * depth, depth)
        far = pltpu.make_async_copy(
            w_hbm.at[rows, pl.ds(pl.multiple_of(other * wide, LANES), wide)],
            w_ref.at[rows, pl.ds(0, wide)],
            w_sems.at[0, n],
        )
        last = pltpu.make_async_copy(
            w_hbm.at[rows, pl.ds(2 * wide, GROUP)], w_ref.at[rows, pl.ds(wide, GROUP)], w_sems.at[1, n]
        )
        far.start()
        last.start()
        copies.append((far, last))
    table_copy.start()
    gain_copy.wait()
    gain = gain_ref[...].astype(jnp.float32)
    x_copy.wait()
    step = 48 if plan.local % 48 == 0 else TILE
    for start in range(0, plan.local, step):
        rows = slice(start, start + step)
        total = jnp.zeros((step, LANES), jnp.float32)
        for n in range(plan.features // LANES):
            part = x_ref[rows, n * LANES : (n + 1) * LANES].astype(jnp.float32)
            total = total + part * part
        mean = jnp.sum(total, axis=-1, keepdims=True) * (1.0 / plan.features)
        scale = lax.rsqrt(mean + norm_eps)
        for n in range(plan.features // LANES):
            columns = slice(n * LANES, (n + 1) * LANES)
            part = x_ref[rows, columns].astype(jnp.float32)
            normed_ref[rows, columns] = (part * scale * gain[n : n + 1, :]).astype(jnp.bfloat16)
    total = None
    for n in range(steps):
        for copy in copies[n]:
            copy.wait()
        rows = slice(n * depth, (n + 1) * depth)
        part = dot(normed_ref[:, rows], w_ref[rows, :])
        total = part if n == 0 else total + part
    mapped = total.astype(jnp.bfloat16)
    table_copy.wait()
    values = dot(mapped[:, wide:], table_ref[:GROUP, :GROUP])
    sub, base = plan.sub, plan.full * plan.local
    turned = [turn_lanes(values, sub * t).astype(jnp.bfloat16) for t in range(plan.rows)]
    lower = other == 0
    for dest in range(plan.rows // 2):
        for h in range(2):
            for quad in range(plan.quads):
                ends = []
                for high in range(2):
                    pieces = []
                    for inner in range(plan.rows):
                        b9 = quad * plan.rows + inner
                        if b9 < plan.half:
                            row = (h * plan.half + b9) * TILE
                            turn = (inner - dest - high * (plan.rows // 2)) % plan.rows
                            pieces.append(turned[turn][row : row + TILE, :])
                    ends.append(by_lane(pieces, sub))
                at = (h * plan.quads + quad) * TILE
                out_ref[dest, base + at : base + at + TILE, :] = jnp.where(lower, ends[0], ends[1])
                near_ref[dest, at : at + TILE, :] = jnp.where(lower, ends[1], ends[0])
    spread(plan, mapped, table_ref, out_ref)


def spread(plan, mapped, table_ref, out_ref):
    for dest in range(plan.rows // 2):
        values = dot(mapped[:, dest * 2 * GROUP : (dest + 1) * 2 * GROUP], table_ref[...])
        for f in range(plan.full):
            out_ref[dest, f * plan.local : (f + 1) * plan.local, :] = values[
                :, f * GROUP : (f + 1) * GROUP
            ].astype(jnp.bfloat16)


def near_kernel(plan, depth, normed_ref, near_ref, w_hbm, table_hbm, out_ref, table_ref, w_ref, sem, w_sems):
    wide = plan.half_wide
    mine = lax.axis_index("row") // (plan.rows // 2)
    steps = plan.features // depth
    copies = []
    for n in range(steps):
        rows = pl.ds(n * depth, depth)
        copy = pltpu.make_async_copy(
            w_hbm.at[rows, pl.ds(pl.multiple_of(mine * wide, LANES), wide)], w_ref.at[rows, :], w_sems.at[n]
        )
        copy.start()
        copies.append(copy)
    table_copy = pltpu.make_async_copy(table_hbm, table_ref, sem)
    table_copy.start()
    out_ref[:, plan.full * plan.local :, :] = near_ref[...]
    total = None
    for n in range(steps):
        copies[n].wait()
        rows = slice(n * depth, (n + 1) * depth)
        part = dot(normed_ref[:, rows], w_ref[rows, :])
        total = part if n == 0 else total + part
    table_copy.wait()
    spread(plan, total.astype(jnp.bfloat16), table_ref, out_ref)


def first_kernel(plan, *refs):
    slabs, (table_ref, out_ref, held_ref) = refs[: plan.rows], refs[plan.rows :]
    row = lax.axis_index("row")
    for s in range(plan.rows):
        held_ref[row ^ s] = slabs[s][...]
    for b9 in range(plan.half):
        quad, inner = divmod(b9, plan.rows)
        columns = []
        for f in range(plan.full):
            parts = []
            for h in range(2):
                at = f * plan.local + (h * plan.half + b9) * TILE
                parts += [held_ref[r, at : at + TILE, :] for r in range(plan.rows)]
            columns.append(jnp.concatenate(parts, axis=0))
        parts = []
        for h in range(2):
            at = plan.full * plan.local + (h * plan.quads + quad) * TILE
            parts += [held_ref[r, at : at + TILE, :] for r in range(plan.rows)]
        columns.append(jnp.concatenate(parts, axis=0))
        result = dot(table_ref[b9], jnp.concatenate(columns, axis=1))
        for f in range(plan.full):
            at = (f * plan.half + b9) * TILE
            piece = result[:, f * LANES : (f + 1) * LANES].astype(jnp.bfloat16)
            for c in range(plan.cols):
                out_ref[c, at : at + TILE, :] = piece[c * TILE : (c + 1) * TILE, :]
        tail = result[:, plan.full * LANES :]
        packed = tail if inner == 0 else jnp.where(lane_index(tail.shape) >= inner * plan.sub, tail, packed)
        if inner == plan.rows - 1 or b9 == plan.half - 1:
            at = (plan.full * plan.half + quad) * TILE
            piece = packed.astype(jnp.bfloat16)
            for c in range(plan.cols):
                out_ref[c, at : at + TILE, :] = piece[c * TILE : (c + 1) * TILE, :]


def second_kernel(plan, scaling, *refs):
    slabs = refs[: plan.cols]
    usual_ref, first_ref, out_ref, held_ref, rhs_ref = refs[plan.cols :]
    row, col = lax.axis_index("row"), lax.axis_index("col")
    for s in range(plan.cols):
        held_ref[col ^ s] = slabs[s][...]
    sub, quarter = plan.sub, TILE // 2
    low = lax.broadcasted_iota(jnp.int32, (TILE, LANES), 0) < quarter
    for b9 in range(plan.half):
        quad, inner = divmod(b9, plan.rows)
        places = [(f * plan.half + b9) * TILE for f in range(plan.full)]
        places.append((plan.full * plan.half + quad) * TILE)
        for p in range(plan.cols // 2):
            at = b9 * (plan.cols // 2) * TILE + p * TILE
            for n, place in enumerate(places):
                even = held_ref[2 * p, place : place + TILE, :].astype(jnp.float32)
                odd = held_ref[2 * p + 1, place : place + TILE, :].astype(jnp.float32)
                both = [
                    jnp.where(low, even, pltpu.roll(odd, quarter, 0)),
                    jnp.where(low, pltpu.roll(even, quarter, 0), odd),
                ]
                for i in range(plan.pairs):
                    value = both[i]
                    if n == plan.full:
                        value = turn_lanes(value, -inner * sub)
                    rhs_ref[i, at : at + TILE, n * LANES : (n + 1) * LANES] = value.astype(jnp.bfloat16)
    wide = (plan.full + 1) * LANES
    lane = lane_index((1, wide))
    last = lane >= plan.full * LANES
    place = jnp.where(last, lane - plan.full * LANES + row * sub, lane & (LANES - 1))
    is_sine = place > GROUP // 2
    span = 2 * plan.block_b
    kept = {}
    for i in range(plan.pairs):
        table = first_ref if i == 0 else usual_ref
        values = rhs_ref[i]
        for r in range(plan.rows):
            cosine = dot(table[0, r * span : (r + 1) * span, :], values)
            sine = dot(table[1, r * span : (r + 1) * span, :], values)
            merged = jnp.where(is_sine, sine, cosine) * scaling
            for f in range(plan.full):
                at = f * plan.out_rows + i * span
                out_ref[r, at : at + span, :] = merged[:, f * LANES : (f + 1) * LANES].astype(jnp.bfloat16)
            tail = merged[:, plan.full * LANES :]
            for t in range(span // TILE):
                whole, inner = divmod(i * (span // TILE) + t, plan.rows)
                at = plan.full * plan.out_rows + whole * TILE
                piece = turn_lanes(tail[t * TILE : (t + 1) * TILE, :], inner * sub)
                if inner:
                    piece = jnp.where(lane_index(piece.shape) >= inner * sub, piece, kept[r])
                kept[r] = piece
                if inner == plan.rows - 1 or (i == plan.pairs - 1 and t == span // TILE - 1):
                    out_ref[r, at : at + TILE, :] = piece.astype(jnp.bfloat16)


def tail_kernel(plan, *refs):
    slabs = refs[: plan.rows]
    unfold_ref, order_ref, w_ref, out_ref, held_ref, spectrum_ref = refs[plan.rows :]
    row = lax.axis_index("row")
    for s in range(plan.rows):
        held_ref[row ^ s] = slabs[s][...]
    order = order_ref[...]
    unfold = unfold_ref[...]
    for q in range(plan.rows):
        pair = [held_ref[q, f * plan.out_rows : (f + 1) * plan.out_rows, :] for f in range(plan.full)]
        ordered = dot(order, jnp.concatenate(pair, axis=1)).astype(jnp.bfloat16)
        spectrum_ref[:, q * 2 * GROUP : (q + 1) * 2 * GROUP] = dot(ordered, unfold).astype(jnp.bfloat16)
    base = plan.full * plan.out_rows
    packed = [held_ref[q, base:, :].astype(jnp.float32) for q in range(plan.rows)]
    turned = [[turn_lanes(value, plan.sub * t) for t in range(plan.rows)] for value in packed]
    pieces = []
    for t in range(plan.row_tiles):
        whole, inner = divmod(t, plan.rows)
        rows = slice(whole * TILE, (whole + 1) * TILE)
        pieces.append(
            by_lane([turned[q][(q - inner) % plan.rows][rows, :] for q in range(plan.rows)], plan.sub)
        )
    last = jnp.concatenate(pieces, axis=0).astype(jnp.bfloat16)
    ordered = dot(order, last).astype(jnp.bfloat16)
    spectrum_ref[:, plan.rows * 2 * GROUP :] = dot(ordered, unfold[:GROUP, :GROUP]).astype(jnp.bfloat16)
    wide = 256
    group = 2 * plan.pairs
    for n in range(plan.features // wide):
        columns = slice(n * wide, (n + 1) * wide)
        result = dot(spectrum_ref[...], w_ref[:, columns]).astype(jnp.bfloat16)
        for k in range(plan.block_b):
            out_ref[k, :, columns] = result[k * group : (k + 1) * group, :]


def estimate(flops, moved):
    return pl.CostEstimate(flops=flops, bytes_accessed=moved, transcendentals=0)


def limit(mebibytes):
    return pltpu.CompilerParams(vmem_limit_bytes=mebibytes * 2**20)


def exchange(values, axis, size):
    here = lax.axis_index(axis)
    out = []
    for s in range(size):
        if isinstance(values, tuple):
            source, index = values[2 * s // size], (here ^ s) % (size // 2)
        else:
            source, index = values, here ^ s
        slab = lax.dynamic_index_in_dim(source, index, 0, keepdims=False)
        if s:
            slab = lax.ppermute(slab, axis, [(n, n ^ s) for n in range(size)])
        out.append(slab)
    return out


def fetch_kernel(w_hbm, after_ref, w_ref, sem):
    copy = pltpu.make_async_copy(w_hbm, w_ref, sem)
    copy.start()
    copy.wait()


def fetch(w_out, after):
    return pl.pallas_call(
        fetch_kernel,
        out_shape=pltpu.VMEM(w_out.shape, w_out.dtype),
        in_specs=[HBM, VMEM],
        out_specs=VMEM,
        scratch_shapes=[pltpu.SemaphoreType.DMA],
        compiler_params=limit(2),
        cost_estimate=estimate(10**9, 2 * w_out.size),
        name="fetch",
    )(pltpu.with_memory_space_constraint(w_out, pltpu.HBM), after)


def packed(plan, tokens, norm_gain, w_in, w_out):
    half_type = jnp.bfloat16
    scaling = 1.0 / math.sqrt(plan.positions * GROUP)
    col = lax.axis_index("col")
    local, features, channels = plan.local, plan.features, plan.channels
    x = tokens.transpose(1, 0, 2).reshape(local, features)
    channel = jnp.asarray(paired(channel_table()), half_type)
    gain = norm_gain.reshape(features // LANES, LANES)
    x, gain, w_in, channel = (pltpu.with_memory_space_constraint(v, pltpu.HBM) for v in (x, gain, w_in, channel))
    depth, wide = features // STEPS, plan.half_wide
    packed_rows = 2 * plan.quads * TILE
    far, near, normed = pl.pallas_call(
        functools.partial(far_kernel, plan, depth),
        out_shape=(
            pltpu.VMEM((plan.rows // 2, plan.send_rows, LANES), half_type),
            pltpu.VMEM((plan.rows // 2, packed_rows, LANES), half_type),
            pltpu.VMEM((local, features), half_type),
        ),
        in_specs=[HBM] * 4,
        out_specs=(VMEM, VMEM, VMEM),
        scratch_shapes=[
            pltpu.VMEM((local, features), half_type),
            pltpu.VMEM((features // LANES, LANES), half_type),
            pltpu.VMEM((2 * GROUP, 2 * GROUP), half_type),
            pltpu.VMEM((features, wide + GROUP), half_type),
            pltpu.SemaphoreType.DMA((3,)),
            pltpu.SemaphoreType.DMA((2, STEPS)),
        ],
        compiler_params=pltpu.CompilerParams(vmem_limit_bytes=16 * 2**20),
        cost_estimate=estimate(local * features * channels, features * channels),
        name="far",
    )(x, gain, w_in, channel)
    close = pl.pallas_call(
        functools.partial(near_kernel, plan, depth),
        out_shape=pltpu.VMEM((plan.rows // 2, plan.send_rows, LANES), half_type),
        in_specs=[VMEM, VMEM, HBM, HBM],
        out_specs=VMEM,
        scratch_shapes=[
            pltpu.VMEM((2 * GROUP, 2 * GROUP), half_type),
            pltpu.VMEM((features, wide), half_type),
            pltpu.SemaphoreType.DMA,
            pltpu.SemaphoreType.DMA((STEPS,)),
        ],
        compiler_params=pltpu.CompilerParams(vmem_limit_bytes=8 * 2**20),
        cost_estimate=estimate(local * features * channels, features * channels),
        name="near",
    )(normed, near, w_in, channel)
    slabs = exchange((close, far), "row", plan.rows)
    first = lax.dynamic_index_in_dim(jnp.asarray(first_tables(plan), half_type), col, 0, keepdims=False)
    turned = pl.pallas_call(
        functools.partial(first_kernel, plan),
        out_shape=jax.ShapeDtypeStruct((plan.cols, plan.tiles * TILE, LANES), half_type),
        in_specs=[VMEM] * (plan.rows + 1),
        out_specs=VMEM,
        scratch_shapes=[pltpu.VMEM((plan.rows, plan.send_rows, LANES), half_type)],
        compiler_params=limit(8),
        cost_estimate=estimate(10**8, 10**6),
        name="first",
    )(*slabs, first)
    slabs = exchange(turned, "col", plan.cols)
    usual, special = (jnp.asarray(table, half_type) for table in second_tables(plan))
    leading = jnp.where(col == 0, special, usual)
    depth = plan.half * plan.cols * 4
    back = pl.pallas_call(
        functools.partial(second_kernel, plan, scaling),
        out_shape=jax.ShapeDtypeStruct((plan.rows, plan.back_rows, LANES), half_type),
        in_specs=[VMEM] * (plan.cols + 2),
        out_specs=VMEM,
        scratch_shapes=[
            pltpu.VMEM((plan.cols, plan.tiles * TILE, LANES), half_type),
            pltpu.VMEM((plan.pairs, depth, (plan.full + 1) * LANES), half_type),
        ],
        compiler_params=limit(12),
        cost_estimate=estimate(3 * 10**8, 10**6),
        name="second",
    )(*slabs, usual, leading)
    slabs = exchange(back, "row", plan.rows)
    w_out = fetch(w_out, slabs[0][:TILE])
    return pl.pallas_call(
        functools.partial(tail_kernel, plan),
        out_shape=jax.ShapeDtypeStruct((plan.block_b, 2 * plan.pairs, features), half_type),
        in_specs=[VMEM] * (plan.rows + 3),
        out_specs=VMEM,
        scratch_shapes=[
            pltpu.VMEM((plan.rows, plan.back_rows, LANES), half_type),
            pltpu.VMEM((plan.out_rows, channels), half_type),
        ],
        compiler_params=limit(12),
        cost_estimate=estimate(2 * local * features * channels, 2 * features * channels),
        name="tail",
    )(*slabs, jnp.asarray(paired(unfold_table()), half_type), jnp.asarray(order_table(plan), half_type), w_out)


def shards(tokens, norm_gain, w_in, w_out):
    rows_first, rows_second, features = tokens.shape
    plan = Plan(
        lax.axis_size("row"), lax.axis_size("col"), rows_first, rows_second, features, w_in.shape[1]
    )
    if plan.fits():
        return packed(plan, tokens, norm_gain, w_in, w_out)
    return general(tokens, norm_gain, w_in, w_out)


def solution(mesh):
    in_specs = (P("row", "col", None), P(), P(), P())
    out_specs = P("row", "col", None)

    return jax.shard_map(shards, mesh=mesh, in_specs=in_specs, out_specs=out_specs, check_vma=False)
```

```python
import functools
import math

import jax
import jax.numpy as jnp
import numpy as np
from jax import lax
from jax.experimental import pallas as pl
from jax.experimental.pallas import tpu as pltpu
from jax.sharding import PartitionSpec as P

GROUP = 128


norm_eps = 1e-06
highest = lax.Precision.HIGHEST


def tables(length):
    series = jnp.arange(length, dtype=jnp.int32)
    product = series[:, None] * series[None, :] % length
    angles = product.astype(jnp.float32) * (2.0 * math.pi / length)
    return (jnp.cos(angles), jnp.sin(angles))


def folded_order(length_first, devices):
    block = length_first // devices
    half_block = block // 2
    series = jnp.arange(length_first, dtype=jnp.int32)
    device = series // block
    inner = series % block
    lower = device * half_block + inner
    upper = length_first - device * half_block - (inner - half_block)
    upper = jnp.where((device == 0) & (inner == half_block), length_first // 2, upper)
    return jnp.where(inner < half_block, lower, upper) % length_first


def to_channels(values, row_count):
    rows_first, rows_second, channels = values.shape
    width = channels // row_count
    parted = values.reshape(rows_first, rows_second, row_count, width).transpose(2, 0, 1, 3)
    return parted.reshape(row_count * rows_first, rows_second * width)


def product(table, values):
    return jnp.dot(table, values, precision=highest)


def middle(real_part, imag_part, width):
    length_first = real_part.shape[0]
    rows_second = real_part.shape[1] // width
    col_count = lax.axis_size("col")
    length_second = rows_second * col_count
    positions = length_first * length_second
    frequency = folded_order(length_first, col_count)
    series = jnp.arange(length_first, dtype=jnp.int32)
    first_angle = (frequency[:, None] * series[None, :] % length_first).astype(jnp.float32)
    first_angle = first_angle * (2.0 * math.pi / length_first)
    first_cos = jnp.cos(first_angle)
    first_sin = jnp.sin(first_angle)
    first_real = product(first_cos, real_part)
    first_imag = -product(first_sin, real_part)
    first_real = first_real + product(first_sin, imag_part)
    first_imag = first_imag + product(first_cos, imag_part)
    first_real = first_real.reshape(length_first, rows_second, width)
    first_imag = first_imag.reshape(length_first, rows_second, width)
    second_index = lax.axis_index("col") * rows_second + jnp.arange(rows_second, dtype=jnp.int32)
    twiddle_angle = (frequency[:, None] * second_index[None, :] % positions).astype(jnp.float32)
    twiddle_angle = twiddle_angle * (2.0 * math.pi / positions)
    twiddle_cos = jnp.cos(twiddle_angle)[:, :, None]
    twiddle_sin = jnp.sin(twiddle_angle)[:, :, None]
    turned_real = first_real * twiddle_cos + first_imag * twiddle_sin
    turned_imag = first_imag * twiddle_cos - first_real * twiddle_sin
    turned = jnp.stack([turned_real, turned_imag]).transpose(0, 2, 1, 3)
    turned = turned.reshape(2, rows_second, length_first * width)
    exchanged = lax.all_to_all(
        turned.astype(jnp.bfloat16), "col", split_axis=2, concat_axis=1, tiled=True
    ).astype(turned.dtype)
    second_cos, second_sin = tables(length_second)
    block = length_first // col_count
    out_shape = (length_second, block, width)
    out_real = (product(second_cos, exchanged[0]) + product(second_sin, exchanged[1])).reshape(
        out_shape
    )
    return out_real


def general(tokens, norm_gain, w_in, w_out):
    rows_first, rows_second, features = tokens.shape
    row_count = lax.axis_size("row")
    length_first = rows_first * row_count
    length_second = rows_second * lax.axis_size("col")
    channels = w_in.shape[1]
    width = channels // row_count
    groups = channels // GROUP
    scaling = 1.0 / math.sqrt(length_first * length_second * GROUP)
    floats = tokens.astype(jnp.float32)
    normed = (
        floats
        * lax.rsqrt(jnp.mean(floats * floats, axis=-1, keepdims=True) + norm_eps)
        * norm_gain.astype(jnp.float32)
    ).astype(jnp.bfloat16)
    mapped = jnp.dot(normed.reshape(-1, features), w_in, preferred_element_type=jnp.float32)
    mapped = mapped.astype(jnp.bfloat16).reshape(rows_first, rows_second, channels)
    channel_cos, channel_sin = tables(GROUP)
    grouped = mapped.astype(jnp.float32).reshape(rows_first, rows_second, groups, GROUP)
    spec_real = jnp.einsum("abgj,jm->abgm", grouped, channel_cos, precision=highest)
    spec_imag = -jnp.einsum("abgj,jm->abgm", grouped, channel_sin, precision=highest)
    stacked = jnp.stack(
        [
            to_channels(spec_real.reshape(rows_first, rows_second, channels), row_count),
            to_channels(spec_imag.reshape(rows_first, rows_second, channels), row_count),
        ]
    )
    arrived = lax.all_to_all(
        stacked.astype(jnp.bfloat16), "row", split_axis=1, concat_axis=1, tiled=True
    ).astype(stacked.dtype)
    result = middle(arrived[0], arrived[1], width)
    spectrum = (result * scaling).astype(jnp.bfloat16)
    returned = lax.all_to_all(spectrum, "row", split_axis=0, concat_axis=2, tiled=True)
    mixed = jnp.dot(returned.reshape(-1, channels), w_out, preferred_element_type=jnp.float32)
    return mixed.astype(jnp.bfloat16).reshape(returned.shape[0], returned.shape[1], features)


LANES = 128
TILE = 8
STEPS = 1
WIDE = 256
VMEM = pl.BlockSpec(memory_space=pltpu.VMEM)
HBM = pl.BlockSpec(memory_space=pltpu.HBM)


class Plan:
    def __init__(self, rows, cols, rows_first, rows_second, features, channels):
        self.rows, self.cols = rows, cols
        self.rows_first, self.rows_second = rows_first, rows_second
        self.features, self.channels = features, channels
        self.length_first = rows_first * rows
        self.length_second = rows_second * cols
        self.positions = self.length_first * self.length_second
        self.groups = channels // GROUP
        self.full = self.groups // rows
        self.sub = GROUP // rows
        self.half = rows_second // 2
        self.quads = -(-self.half // rows)
        self.tiles = self.full * self.half + self.quads
        self.local = rows_first * rows_second
        self.half_wide = rows // 2 * self.full * GROUP
        self.send_rows = self.full * self.local + 2 * self.quads * TILE
        self.pairs = self.length_first // cols // 2
        self.block_b = self.length_second // rows
        self.out_rows = self.block_b * 2 * self.pairs
        self.row_tiles = self.out_rows // TILE
        self.back_quads = -(-self.row_tiles // rows)
        self.back_rows = self.full * self.out_rows + self.back_quads * TILE

    def fits(self):
        return (
            GROUP == LANES
            and self.rows & (self.rows - 1) == 0
            and self.cols & (self.cols - 1) == 0
            and 1 < self.rows <= 8
            and self.cols > 1
            and self.rows_first == TILE
            and self.rows_second % 2 == 0
            and self.channels % GROUP == 0
            and self.groups % self.rows == 1
            and self.full == 2
            and self.length_first == 4 * self.cols
            and self.length_second % self.rows == 0
            and 2 * self.block_b % TILE == 0
            and self.features % 512 == 0
        )


def channel_table():
    j = np.arange(GROUP)[:, None]
    u = np.arange(GROUP)[None, :]
    half = GROUP // 2
    m = np.where(u <= half, u, u - half)
    angle = 2.0 * np.pi * (j * m % GROUP) / GROUP
    return np.where(u <= half, np.cos(angle), np.sin(angle))


def unfold_table():
    half = GROUP // 2
    table = np.zeros((GROUP, GROUP))
    for m in range(GROUP):
        near = m if m <= half else GROUP - m
        table[near, m] = 1.0
        if 0 < near < half:
            table[half + near, m] = -1.0 if m < half else 1.0
    return table


def paired(table):
    zero = np.zeros_like(table)
    return np.block([[table, zero], [zero, table]])


def first_tables(plan):
    a = np.arange(plan.length_first)
    out = np.zeros((plan.cols, plan.half, plan.cols, plan.pairs, 2, 2, 2, plan.length_first))
    for col in range(plan.cols):
        for b9 in range(plan.half):
            for h in range(2):
                b = col * plan.rows_second + h * plan.half + b9
                for c in range(plan.cols):
                    for i in range(plan.pairs):
                        k = c * plan.pairs + i
                        if k == 0:
                            out[col, b9, c, i, h, 0, h] = 1.0
                            out[col, b9, c, i, h, 1, h] = np.where(a % 2 == 0, 1.0, -1.0)
                        else:
                            phase = (a * plan.length_second + b) * k % plan.positions
                            angle = 2.0 * np.pi * phase / plan.positions
                            out[col, b9, c, i, h, 0, h] = np.cos(angle)
                            out[col, b9, c, i, h, 1, h] = -np.sin(angle)
    size = 2 * plan.length_first
    return out.reshape(plan.cols, plan.half, size, size)


def second_tables(plan):
    length = plan.length_second
    b9 = np.arange(plan.half)[:, None, None]
    c = np.arange(plan.cols)[None, :, None]
    h = np.arange(2)[None, None, :]
    b = (c * plan.rows_second + h * plan.half + b9).reshape(-1)
    k = np.arange(length)
    angle = 2.0 * np.pi * (k[:, None] * b[None, :] % length) / length
    cos, sin = np.cos(angle), np.sin(angle)
    cosine = np.stack([cos, sin], axis=-1)
    sine = np.stack([sin, -cos], axis=-1)

    def arrange(plus, minus):
        both = np.stack([plus, minus]).reshape(2, plan.rows, plan.block_b, -1)
        return both.transpose(1, 0, 2, 3).reshape(2 * length, -1)

    usual = np.stack([arrange(cosine, cosine[::-1]), arrange(sine, -sine[::-1])])
    turn = 2.0 * np.pi * ((plan.length_first // 2) * b % plan.positions) / plan.positions
    late = angle + turn[None, :]
    zero = np.zeros_like(cos)
    first = np.stack(
        [
            arrange(np.stack([cos, zero], -1), np.stack([zero, np.cos(late)], -1)),
            arrange(np.stack([sin, zero], -1), np.stack([zero, np.sin(late)], -1)),
        ]
    )
    return usual, first


def order_table(plan):
    table = np.zeros((plan.out_rows, plan.out_rows))
    for i in range(plan.pairs):
        for neg in range(2):
            for k in range(plan.block_b):
                row = (k * 2 + neg) * plan.pairs + i
                table[row, (i * 2 + neg) * plan.block_b + k] = 1.0
    return table


def dot(left, right):
    return jnp.dot(left, right, preferred_element_type=jnp.float32)


def lane_index(shape):
    return lax.broadcasted_iota(jnp.int32, shape, 1)


def turn_lanes(value, amount):
    amount = amount % LANES
    return value if amount == 0 else pltpu.roll(value, amount, 1)


def by_lane(pieces, sub):
    out = pieces[0]
    lane = lane_index(out.shape)
    for n in range(1, len(pieces)):
        out = jnp.where(lane >= n * sub, pieces[n], out)
    return out


def far_kernel(
    plan, depth, x_hbm, gain_hbm, w_hbm, table_hbm, out_ref, near_ref, normed_ref, x_ref, gain_ref, table_ref, w_ref, sems, w_sems
):
    wide = plan.half_wide
    other = 1 - lax.axis_index("row") // (plan.rows // 2)
    x_copy = pltpu.make_async_copy(x_hbm, x_ref, sems.at[0])
    gain_copy = pltpu.make_async_copy(gain_hbm, gain_ref, sems.at[1])
    table_copy = pltpu.make_async_copy(table_hbm, table_ref, sems.at[2])
    x_copy.start()
    gain_copy.start()
    steps = plan.features // depth
    copies = []
    for n in range(steps):
        rows = pl.ds(n * depth, depth)
        far = pltpu.make_async_copy(
            w_hbm.at[rows, pl.ds(pl.multiple_of(other * wide, LANES), wide)],
            w_ref.at[rows, pl.ds(0, wide)],
            w_sems.at[0, n],
        )
        last = pltpu.make_async_copy(
            w_hbm.at[rows, pl.ds(2 * wide, GROUP)], w_ref.at[rows, pl.ds(wide, GROUP)], w_sems.at[1, n]
        )
        far.start()
        last.start()
        copies.append((far, last))
    table_copy.start()
    gain_copy.wait()
    gain = gain_ref[...].astype(jnp.float32)
    x_copy.wait()
    step = 48 if plan.local % 48 == 0 else TILE
    for start in range(0, plan.local, step):
        rows = slice(start, start + step)
        total = jnp.zeros((step, LANES), jnp.float32)
        for n in range(plan.features // LANES):
            part = x_ref[rows, n * LANES : (n + 1) * LANES].astype(jnp.float32)
            total = total + part * part
        mean = jnp.sum(total, axis=-1, keepdims=True) * (1.0 / plan.features)
        scale = lax.rsqrt(mean + norm_eps)
        for n in range(plan.features // LANES):
            columns = slice(n * LANES, (n + 1) * LANES)
            part = x_ref[rows, columns].astype(jnp.float32)
            normed_ref[rows, columns] = (part * scale * gain[n : n + 1, :]).astype(jnp.bfloat16)
    total = None
    for n in range(steps):
        for copy in copies[n]:
            copy.wait()
        rows = slice(n * depth, (n + 1) * depth)
        part = dot(normed_ref[:, rows], w_ref[rows, :])
        total = part if n == 0 else total + part
    mapped = total.astype(jnp.bfloat16)
    table_copy.wait()
    values = dot(mapped[:, wide:], table_ref[:GROUP, :GROUP])
    sub, base = plan.sub, plan.full * plan.local
    turned = [turn_lanes(values, sub * t).astype(jnp.bfloat16) for t in range(plan.rows)]
    lower = other == 0
    for dest in range(plan.rows // 2):
        for h in range(2):
            for quad in range(plan.quads):
                ends = []
                for high in range(2):
                    pieces = []
                    for inner in range(plan.rows):
                        b9 = quad * plan.rows + inner
                        if b9 < plan.half:
                            row = (h * plan.half + b9) * TILE
                            turn = (inner - dest - high * (plan.rows // 2)) % plan.rows
                            pieces.append(turned[turn][row : row + TILE, :])
                    ends.append(by_lane(pieces, sub))
                at = (h * plan.quads + quad) * TILE
                out_ref[dest, base + at : base + at + TILE, :] = jnp.where(lower, ends[0], ends[1])
                near_ref[dest, at : at + TILE, :] = jnp.where(lower, ends[1], ends[0])
    spread(plan, mapped, table_ref, out_ref)


def spread(plan, mapped, table_ref, out_ref):
    for dest in range(plan.rows // 2):
        values = dot(mapped[:, dest * 2 * GROUP : (dest + 1) * 2 * GROUP], table_ref[...])
        for f in range(plan.full):
            out_ref[dest, f * plan.local : (f + 1) * plan.local, :] = values[
                :, f * GROUP : (f + 1) * GROUP
            ].astype(jnp.bfloat16)


def near_kernel(plan, depth, normed_ref, near_ref, w_hbm, table_hbm, out_ref, table_ref, w_ref, sem, w_sems):
    wide = plan.half_wide
    mine = lax.axis_index("row") // (plan.rows // 2)
    steps = plan.features // depth
    copies = []
    for n in range(steps):
        rows = pl.ds(n * depth, depth)
        copy = pltpu.make_async_copy(
            w_hbm.at[rows, pl.ds(pl.multiple_of(mine * wide, LANES), wide)], w_ref.at[rows, :], w_sems.at[n]
        )
        copy.start()
        copies.append(copy)
    table_copy = pltpu.make_async_copy(table_hbm, table_ref, sem)
    table_copy.start()
    out_ref[:, plan.full * plan.local :, :] = near_ref[...]
    total = None
    for n in range(steps):
        copies[n].wait()
        rows = slice(n * depth, (n + 1) * depth)
        part = dot(normed_ref[:, rows], w_ref[rows, :])
        total = part if n == 0 else total + part
    table_copy.wait()
    spread(plan, total.astype(jnp.bfloat16), table_ref, out_ref)


def first_kernel(plan, *refs):
    slabs, (table_ref, out_ref, held_ref) = refs[: plan.rows], refs[plan.rows :]
    row = lax.axis_index("row")
    for s in range(plan.rows):
        held_ref[row ^ s] = slabs[s][...]
    for b9 in range(plan.half):
        quad, inner = divmod(b9, plan.rows)
        columns = []
        for f in range(plan.full):
            parts = []
            for h in range(2):
                at = f * plan.local + (h * plan.half + b9) * TILE
                parts += [held_ref[r, at : at + TILE, :] for r in range(plan.rows)]
            columns.append(jnp.concatenate(parts, axis=0))
        parts = []
        for h in range(2):
            at = plan.full * plan.local + (h * plan.quads + quad) * TILE
            parts += [held_ref[r, at : at + TILE, :] for r in range(plan.rows)]
        columns.append(jnp.concatenate(parts, axis=0))
        result = dot(table_ref[b9], jnp.concatenate(columns, axis=1))
        for f in range(plan.full):
            at = (f * plan.half + b9) * TILE
            piece = result[:, f * LANES : (f + 1) * LANES].astype(jnp.bfloat16)
            for c in range(plan.cols):
                out_ref[c, at : at + TILE, :] = piece[c * TILE : (c + 1) * TILE, :]
        tail = result[:, plan.full * LANES :]
        packed = tail if inner == 0 else jnp.where(lane_index(tail.shape) >= inner * plan.sub, tail, packed)
        if inner == plan.rows - 1 or b9 == plan.half - 1:
            at = (plan.full * plan.half + quad) * TILE
            piece = packed.astype(jnp.bfloat16)
            for c in range(plan.cols):
                out_ref[c, at : at + TILE, :] = piece[c * TILE : (c + 1) * TILE, :]


def second_kernel(plan, scaling, *refs):
    slabs = refs[: plan.cols]
    usual_ref, first_ref, out_ref, held_ref, rhs_ref = refs[plan.cols :]
    row, col = lax.axis_index("row"), lax.axis_index("col")
    for s in range(plan.cols):
        held_ref[col ^ s] = slabs[s][...]
    sub, quarter = plan.sub, TILE // 2
    low = lax.broadcasted_iota(jnp.int32, (TILE, LANES), 0) < quarter
    for b9 in range(plan.half):
        quad, inner = divmod(b9, plan.rows)
        places = [(f * plan.half + b9) * TILE for f in range(plan.full)]
        places.append((plan.full * plan.half + quad) * TILE)
        for p in range(plan.cols // 2):
            at = b9 * (plan.cols // 2) * TILE + p * TILE
            for n, place in enumerate(places):
                even = held_ref[2 * p, place : place + TILE, :].astype(jnp.float32)
                odd = held_ref[2 * p + 1, place : place + TILE, :].astype(jnp.float32)
                both = [
                    jnp.where(low, even, pltpu.roll(odd, quarter, 0)),
                    jnp.where(low, pltpu.roll(even, quarter, 0), odd),
                ]
                for i in range(plan.pairs):
                    value = both[i]
                    if n == plan.full:
                        value = turn_lanes(value, -inner * sub)
                    rhs_ref[i, at : at + TILE, n * LANES : (n + 1) * LANES] = value.astype(jnp.bfloat16)
    wide = (plan.full + 1) * LANES
    lane = lane_index((1, wide))
    last = lane >= plan.full * LANES
    place = jnp.where(last, lane - plan.full * LANES + row * sub, lane & (LANES - 1))
    is_sine = place > GROUP // 2
    span = 2 * plan.block_b
    total = plan.rows * span
    tails = {}
    for i in range(plan.pairs):
        table = first_ref if i == 0 else usual_ref
        both = dot(table[...], rhs_ref[i])
        for r in range(plan.rows):
            cosine, sine = both[r * span : (r + 1) * span, :], both[total + r * span : total + (r + 1) * span, :]
            merged = jnp.where(is_sine, sine, cosine) * scaling
            for f in range(plan.full):
                at = f * plan.out_rows + i * span
                out_ref[r, at : at + span, :] = merged[:, f * LANES : (f + 1) * LANES].astype(jnp.bfloat16)
            tails[i, r] = merged[:, plan.full * LANES :]
    for r in range(plan.rows):
        pieces = []
        for t in range(plan.row_tiles):
            i, at = divmod(t * TILE, span)
            pieces.append(turn_lanes(tails[i, r][at : at + TILE, :], (t % plan.rows) * sub))
        for whole in range(plan.back_quads):
            at = plan.full * plan.out_rows + whole * TILE
            group = pieces[whole * plan.rows : (whole + 1) * plan.rows]
            out_ref[r, at : at + TILE, :] = by_lane(group, sub).astype(jnp.bfloat16)


def unfolded(plan, order, unfold, slabs):
    pair = [slabs[f * plan.out_rows : (f + 1) * plan.out_rows, :] for f in range(plan.full)]
    ordered = dot(order, jnp.concatenate(pair, axis=1)).astype(jnp.bfloat16)
    return dot(ordered, unfold).astype(jnp.bfloat16)


def early_kernel(plan, slab_ref, unfold_ref, order_ref, w_hbm, partial_ref, w_ref, own_ref, sems):
    row = lax.axis_index("row")
    each = plan.full * GROUP

    def part(s):
        return w_hbm.at[pl.ds(pl.multiple_of((row ^ s) * each, LANES), each), :]

    copies = [pltpu.make_async_copy(part(0), own_ref, sems.at[0])]
    for s in range(1, plan.rows):
        copies.append(pltpu.make_async_copy(part(s), w_ref.at[pl.ds((s - 1) * each, each), :], sems.at[s]))
    copies.append(
        pltpu.make_async_copy(
            w_hbm.at[pl.ds(plan.rows * each, GROUP), :],
            w_ref.at[pl.ds((plan.rows - 1) * each, GROUP), :],
            sems.at[plan.rows],
        )
    )
    for copy in copies:
        copy.start()
    spectrum = unfolded(plan, order_ref[...], unfold_ref[...], slab_ref)
    copies[0].wait()
    for n in range(plan.features // WIDE):
        columns = slice(n * WIDE, (n + 1) * WIDE)
        partial_ref[:, columns] = dot(spectrum, own_ref[:, columns])
    for copy in copies[1:]:
        copy.wait()


def tail_kernel(plan, *refs):
    slabs = refs[: plan.rows]
    unfold_ref, order_ref, partial_ref, w_ref, out_hbm, packed_ref, stage_ref, sems = refs[plan.rows :]
    row = lax.axis_index("row")
    main = plan.full * plan.out_rows
    for s in range(plan.rows):
        packed_ref[row ^ s] = slabs[s][main:, :]
    order, unfold = order_ref[...], unfold_ref[...]
    spectrum = [unfolded(plan, order, unfold, slabs[s]) for s in range(1, plan.rows)]
    packed = [packed_ref[q].astype(jnp.float32) for q in range(plan.rows)]
    turned = [[turn_lanes(value, plan.sub * t) for t in range(plan.rows)] for value in packed]
    pieces = []
    for t in range(plan.row_tiles):
        whole, inner = divmod(t, plan.rows)
        rows = slice(whole * TILE, (whole + 1) * TILE)
        pieces.append(
            by_lane([turned[q][(q - inner) % plan.rows][rows, :] for q in range(plan.rows)], plan.sub)
        )
    last = jnp.concatenate(pieces, axis=0).astype(jnp.bfloat16)
    ordered = dot(order, last).astype(jnp.bfloat16)
    spectrum.append(dot(ordered, unfold[:GROUP, :GROUP]).astype(jnp.bfloat16))
    spectrum = jnp.concatenate(spectrum, axis=1)
    group = 2 * plan.pairs
    copies = []
    for n in range(plan.features // WIDE):
        columns = slice(n * WIDE, (n + 1) * WIDE)
        result = (partial_ref[:, columns] + dot(spectrum, w_ref[:, columns])).astype(jnp.bfloat16)
        for k in range(plan.block_b):
            stage_ref[n, k] = result[k * group : (k + 1) * group, :]
        copy = pltpu.make_async_copy(stage_ref.at[n], out_hbm.at[:, :, pl.ds(n * WIDE, WIDE)], sems.at[n])
        copy.start()
        copies.append(copy)
    for copy in copies:
        copy.wait()


def estimate(flops, moved):
    return pl.CostEstimate(flops=flops, bytes_accessed=moved, transcendentals=0)


def limit(mebibytes):
    return pltpu.CompilerParams(vmem_limit_bytes=mebibytes * 2**20)


def exchange(values, axis, size):
    here = lax.axis_index(axis)
    out = []
    for s in range(size):
        if isinstance(values, tuple):
            source, index = values[2 * s // size], (here ^ s) % (size // 2)
        else:
            source, index = values, here ^ s
        slab = lax.dynamic_index_in_dim(source, index, 0, keepdims=False)
        if s:
            slab = lax.ppermute(slab, axis, [(n, n ^ s) for n in range(size)])
        out.append(slab)
    return out


def packed(plan, tokens, norm_gain, w_in, w_out):
    half_type = jnp.bfloat16
    scaling = 1.0 / math.sqrt(plan.positions * GROUP)
    col = lax.axis_index("col")
    local, features, channels = plan.local, plan.features, plan.channels
    x = tokens.transpose(1, 0, 2).reshape(local, features)
    channel = jnp.asarray(paired(channel_table()), half_type)
    gain = norm_gain.reshape(features // LANES, LANES)
    x, gain, w_in, channel = (pltpu.with_memory_space_constraint(v, pltpu.HBM) for v in (x, gain, w_in, channel))
    depth, wide = features // STEPS, plan.half_wide
    packed_rows = 2 * plan.quads * TILE
    far, near, normed = pl.pallas_call(
        functools.partial(far_kernel, plan, depth),
        out_shape=(
            pltpu.VMEM((plan.rows // 2, plan.send_rows, LANES), half_type),
            pltpu.VMEM((plan.rows // 2, packed_rows, LANES), half_type),
            pltpu.VMEM((local, features), half_type),
        ),
        in_specs=[HBM] * 4,
        out_specs=(VMEM, VMEM, VMEM),
        scratch_shapes=[
            pltpu.VMEM((local, features), half_type),
            pltpu.VMEM((features // LANES, LANES), half_type),
            pltpu.VMEM((2 * GROUP, 2 * GROUP), half_type),
            pltpu.VMEM((features, wide + GROUP), half_type),
            pltpu.SemaphoreType.DMA((3,)),
            pltpu.SemaphoreType.DMA((2, STEPS)),
        ],
        compiler_params=pltpu.CompilerParams(vmem_limit_bytes=16 * 2**20),
        cost_estimate=estimate(local * features * channels, features * channels),
        name="far",
    )(x, gain, w_in, channel)
    close = pl.pallas_call(
        functools.partial(near_kernel, plan, depth),
        out_shape=pltpu.VMEM((plan.rows // 2, plan.send_rows, LANES), half_type),
        in_specs=[VMEM, VMEM, HBM, HBM],
        out_specs=VMEM,
        scratch_shapes=[
            pltpu.VMEM((2 * GROUP, 2 * GROUP), half_type),
            pltpu.VMEM((features, wide), half_type),
            pltpu.SemaphoreType.DMA,
            pltpu.SemaphoreType.DMA((STEPS,)),
        ],
        compiler_params=pltpu.CompilerParams(vmem_limit_bytes=8 * 2**20),
        cost_estimate=estimate(local * features * channels, features * channels),
        name="near",
    )(normed, near, w_in, channel)
    slabs = exchange((close, far), "row", plan.rows)
    first = lax.dynamic_index_in_dim(jnp.asarray(first_tables(plan), half_type), col, 0, keepdims=False)
    turned = pl.pallas_call(
        functools.partial(first_kernel, plan),
        out_shape=jax.ShapeDtypeStruct((plan.cols, plan.tiles * TILE, LANES), half_type),
        in_specs=[VMEM] * (plan.rows + 1),
        out_specs=VMEM,
        scratch_shapes=[pltpu.VMEM((plan.rows, plan.send_rows, LANES), half_type)],
        compiler_params=limit(8),
        cost_estimate=estimate(10**8, 10**6),
        name="first",
    )(*slabs, first)
    slabs = exchange(turned, "col", plan.cols)
    usual, special = (jnp.asarray(table, half_type) for table in second_tables(plan))
    usual, special = (table.reshape(-1, table.shape[-1]) for table in (usual, special))
    leading = jnp.where(col == 0, special, usual)
    depth = plan.half * plan.cols * 4
    back = pl.pallas_call(
        functools.partial(second_kernel, plan, scaling),
        out_shape=jax.ShapeDtypeStruct((plan.rows, plan.back_rows, LANES), half_type),
        in_specs=[VMEM] * (plan.cols + 2),
        out_specs=VMEM,
        scratch_shapes=[
            pltpu.VMEM((plan.cols, plan.tiles * TILE, LANES), half_type),
            pltpu.VMEM((plan.pairs, depth, (plan.full + 1) * LANES), half_type),
        ],
        compiler_params=limit(12),
        cost_estimate=estimate(3 * 10**8, 10**6),
        name="second",
    )(*slabs, usual, leading)
    slabs = exchange(back, "row", plan.rows)
    unfold = jnp.asarray(paired(unfold_table()), half_type)
    order = jnp.asarray(order_table(plan), half_type)
    main, each = plan.full * plan.out_rows, plan.full * GROUP
    cost = estimate(local * features * channels, features * channels)
    partial, w_rest = pl.pallas_call(
        functools.partial(early_kernel, plan),
        out_shape=(
            pltpu.VMEM((plan.out_rows, features), jnp.float32),
            pltpu.VMEM((channels - each, features), half_type),
        ),
        in_specs=[VMEM] * 3 + [HBM],
        out_specs=(VMEM, VMEM),
        scratch_shapes=[pltpu.VMEM((each, features), half_type), pltpu.SemaphoreType.DMA((plan.rows + 1,))],
        compiler_params=limit(8),
        cost_estimate=cost,
        name="early",
    )(slabs[0], unfold, order, pltpu.with_memory_space_constraint(w_out, pltpu.HBM))
    return pl.pallas_call(
        functools.partial(tail_kernel, plan),
        out_shape=jax.ShapeDtypeStruct((plan.block_b, 2 * plan.pairs, features), half_type),
        in_specs=[VMEM] * (plan.rows + 4),
        out_specs=HBM,
        scratch_shapes=[
            pltpu.VMEM((plan.rows, plan.back_rows - main, LANES), half_type),
            pltpu.VMEM((features // WIDE, plan.block_b, 2 * plan.pairs, WIDE), half_type),
            pltpu.SemaphoreType.DMA((features // WIDE,)),
        ],
        compiler_params=limit(12),
        cost_estimate=cost,
        name="tail",
    )(*slabs, unfold, order, partial, w_rest)


def shards(tokens, norm_gain, w_in, w_out):
    rows_first, rows_second, features = tokens.shape
    plan = Plan(
        lax.axis_size("row"), lax.axis_size("col"), rows_first, rows_second, features, w_in.shape[1]
    )
    if plan.fits():
        return packed(plan, tokens, norm_gain, w_in, w_out)
    return general(tokens, norm_gain, w_in, w_out)


def solution(mesh):
    in_specs = (P("row", "col", None), P(), P(), P())
    out_specs = P("row", "col", None)

    return jax.shard_map(shards, mesh=mesh, in_specs=in_specs, out_specs=out_specs, check_vma=False)
```

```python
import functools
import math

import jax
import jax.numpy as jnp
import numpy as np
from jax import lax
from jax.experimental import pallas as pl
from jax.experimental.pallas import tpu as pltpu
from jax.sharding import PartitionSpec as P

GROUP = 128


norm_eps = 1e-06
highest = lax.Precision.HIGHEST


def tables(length):
    series = jnp.arange(length, dtype=jnp.int32)
    product = series[:, None] * series[None, :] % length
    angles = product.astype(jnp.float32) * (2.0 * math.pi / length)
    return (jnp.cos(angles), jnp.sin(angles))


def folded_order(length_first, devices):
    block = length_first // devices
    half_block = block // 2
    series = jnp.arange(length_first, dtype=jnp.int32)
    device = series // block
    inner = series % block
    lower = device * half_block + inner
    upper = length_first - device * half_block - (inner - half_block)
    upper = jnp.where((device == 0) & (inner == half_block), length_first // 2, upper)
    return jnp.where(inner < half_block, lower, upper) % length_first


def to_channels(values, row_count):
    rows_first, rows_second, channels = values.shape
    width = channels // row_count
    parted = values.reshape(rows_first, rows_second, row_count, width).transpose(2, 0, 1, 3)
    return parted.reshape(row_count * rows_first, rows_second * width)


def product(table, values):
    return jnp.dot(table, values, precision=highest)


def middle(real_part, imag_part, width):
    length_first = real_part.shape[0]
    rows_second = real_part.shape[1] // width
    col_count = lax.axis_size("col")
    length_second = rows_second * col_count
    positions = length_first * length_second
    frequency = folded_order(length_first, col_count)
    series = jnp.arange(length_first, dtype=jnp.int32)
    first_angle = (frequency[:, None] * series[None, :] % length_first).astype(jnp.float32)
    first_angle = first_angle * (2.0 * math.pi / length_first)
    first_cos = jnp.cos(first_angle)
    first_sin = jnp.sin(first_angle)
    first_real = product(first_cos, real_part)
    first_imag = -product(first_sin, real_part)
    first_real = first_real + product(first_sin, imag_part)
    first_imag = first_imag + product(first_cos, imag_part)
    first_real = first_real.reshape(length_first, rows_second, width)
    first_imag = first_imag.reshape(length_first, rows_second, width)
    second_index = lax.axis_index("col") * rows_second + jnp.arange(rows_second, dtype=jnp.int32)
    twiddle_angle = (frequency[:, None] * second_index[None, :] % positions).astype(jnp.float32)
    twiddle_angle = twiddle_angle * (2.0 * math.pi / positions)
    twiddle_cos = jnp.cos(twiddle_angle)[:, :, None]
    twiddle_sin = jnp.sin(twiddle_angle)[:, :, None]
    turned_real = first_real * twiddle_cos + first_imag * twiddle_sin
    turned_imag = first_imag * twiddle_cos - first_real * twiddle_sin
    turned = jnp.stack([turned_real, turned_imag]).transpose(0, 2, 1, 3)
    turned = turned.reshape(2, rows_second, length_first * width)
    exchanged = lax.all_to_all(
        turned.astype(jnp.bfloat16), "col", split_axis=2, concat_axis=1, tiled=True
    ).astype(turned.dtype)
    second_cos, second_sin = tables(length_second)
    block = length_first // col_count
    out_shape = (length_second, block, width)
    out_real = (product(second_cos, exchanged[0]) + product(second_sin, exchanged[1])).reshape(
        out_shape
    )
    return out_real


def general(tokens, norm_gain, w_in, w_out):
    rows_first, rows_second, features = tokens.shape
    row_count = lax.axis_size("row")
    length_first = rows_first * row_count
    length_second = rows_second * lax.axis_size("col")
    channels = w_in.shape[1]
    width = channels // row_count
    groups = channels // GROUP
    scaling = 1.0 / math.sqrt(length_first * length_second * GROUP)
    floats = tokens.astype(jnp.float32)
    normed = (
        floats
        * lax.rsqrt(jnp.mean(floats * floats, axis=-1, keepdims=True) + norm_eps)
        * norm_gain.astype(jnp.float32)
    ).astype(jnp.bfloat16)
    mapped = jnp.dot(normed.reshape(-1, features), w_in, preferred_element_type=jnp.float32)
    mapped = mapped.astype(jnp.bfloat16).reshape(rows_first, rows_second, channels)
    channel_cos, channel_sin = tables(GROUP)
    grouped = mapped.astype(jnp.float32).reshape(rows_first, rows_second, groups, GROUP)
    spec_real = jnp.einsum("abgj,jm->abgm", grouped, channel_cos, precision=highest)
    spec_imag = -jnp.einsum("abgj,jm->abgm", grouped, channel_sin, precision=highest)
    stacked = jnp.stack(
        [
            to_channels(spec_real.reshape(rows_first, rows_second, channels), row_count),
            to_channels(spec_imag.reshape(rows_first, rows_second, channels), row_count),
        ]
    )
    arrived = lax.all_to_all(
        stacked.astype(jnp.bfloat16), "row", split_axis=1, concat_axis=1, tiled=True
    ).astype(stacked.dtype)
    result = middle(arrived[0], arrived[1], width)
    spectrum = (result * scaling).astype(jnp.bfloat16)
    returned = lax.all_to_all(spectrum, "row", split_axis=0, concat_axis=2, tiled=True)
    mixed = jnp.dot(returned.reshape(-1, channels), w_out, preferred_element_type=jnp.float32)
    return mixed.astype(jnp.bfloat16).reshape(returned.shape[0], returned.shape[1], features)


LANES = 128
TILE = 8
STEPS = 1
WIDE = 256
CROSS = ((0, 0), (7, 7), (6, 6), (5, 3), (4, 2), (3, 5), (2, 4), (1, 1))
VMEM = pl.BlockSpec(memory_space=pltpu.VMEM)
HBM = pl.BlockSpec(memory_space=pltpu.HBM)


class Plan:
    def __init__(self, rows, cols, rows_first, rows_second, features, channels):
        self.rows, self.cols = rows, cols
        self.rows_first, self.rows_second = rows_first, rows_second
        self.features, self.channels = features, channels
        self.length_first = rows_first * rows
        self.length_second = rows_second * cols
        self.positions = self.length_first * self.length_second
        self.groups = channels // GROUP
        self.full = self.groups // rows
        self.sub = GROUP // rows
        self.half = rows_second // 2
        self.quads = -(-self.half // rows)
        self.tiles = self.full * self.half + self.quads
        self.local = rows_first * rows_second
        self.half_wide = rows // 2 * self.full * GROUP
        self.send_rows = self.full * self.local + 2 * self.quads * TILE
        self.pairs = self.length_first // cols // 2
        self.block_b = self.length_second // rows
        self.out_rows = self.block_b * 2 * self.pairs
        self.row_tiles = self.out_rows // TILE
        self.back_quads = -(-self.row_tiles // rows)
        self.back_rows = self.full * self.out_rows + self.back_quads * TILE

    def fits(self):
        return (
            GROUP == LANES
            and self.rows & (self.rows - 1) == 0
            and self.cols & (self.cols - 1) == 0
            and 1 < self.rows <= 8
            and self.cols > 1
            and self.rows_first == TILE
            and self.rows_second % 2 == 0
            and self.channels % GROUP == 0
            and self.groups % self.rows == 1
            and self.full == 2
            and self.length_first == 4 * self.cols
            and self.length_second % self.rows == 0
            and 2 * self.block_b % TILE == 0
            and self.features % 512 == 0
        )


def channel_table():
    j = np.arange(GROUP)[:, None]
    u = np.arange(GROUP)[None, :]
    half = GROUP // 2
    m = np.where(u <= half, u, u - half)
    angle = 2.0 * np.pi * (j * m % GROUP) / GROUP
    return np.where(u <= half, np.cos(angle), np.sin(angle))


def unfold_table():
    half = GROUP // 2
    table = np.zeros((GROUP, GROUP))
    for m in range(GROUP):
        near = m if m <= half else GROUP - m
        table[near, m] = 1.0
        if 0 < near < half:
            table[half + near, m] = -1.0 if m < half else 1.0
    return table


def paired(table):
    zero = np.zeros_like(table)
    return np.block([[table, zero], [zero, table]])


def first_tables(plan):
    a = np.arange(plan.length_first)
    out = np.zeros((plan.cols, plan.half, plan.cols, plan.pairs, 2, 2, 2, plan.length_first))
    for col in range(plan.cols):
        for b9 in range(plan.half):
            for h in range(2):
                b = col * plan.rows_second + h * plan.half + b9
                for c in range(plan.cols):
                    for i in range(plan.pairs):
                        k = c * plan.pairs + i
                        if k == 0:
                            out[col, b9, c, i, h, 0, h] = 1.0
                            out[col, b9, c, i, h, 1, h] = np.where(a % 2 == 0, 1.0, -1.0)
                        else:
                            phase = (a * plan.length_second + b) * k % plan.positions
                            angle = 2.0 * np.pi * phase / plan.positions
                            out[col, b9, c, i, h, 0, h] = np.cos(angle)
                            out[col, b9, c, i, h, 1, h] = -np.sin(angle)
    size = 2 * plan.length_first
    return out.reshape(plan.cols, plan.half, size, size)


def second_tables(plan):
    length = plan.length_second
    b9 = np.arange(plan.half)[:, None, None]
    c = np.arange(plan.cols)[None, :, None]
    h = np.arange(2)[None, None, :]
    b = (c * plan.rows_second + h * plan.half + b9).reshape(-1)
    k = np.arange(length)
    angle = 2.0 * np.pi * (k[:, None] * b[None, :] % length) / length
    cos, sin = np.cos(angle), np.sin(angle)
    cosine = np.stack([cos, sin], axis=-1)
    sine = np.stack([sin, -cos], axis=-1)

    def arrange(plus, minus):
        both = np.stack([plus, minus]).reshape(2, plan.rows, plan.block_b, -1)
        return both.transpose(1, 0, 2, 3).reshape(2 * length, -1)

    usual = np.stack([arrange(cosine, cosine[::-1]), arrange(sine, -sine[::-1])])
    turn = 2.0 * np.pi * ((plan.length_first // 2) * b % plan.positions) / plan.positions
    late = angle + turn[None, :]
    zero = np.zeros_like(cos)
    first = np.stack(
        [
            arrange(np.stack([cos, zero], -1), np.stack([zero, np.cos(late)], -1)),
            arrange(np.stack([sin, zero], -1), np.stack([zero, np.sin(late)], -1)),
        ]
    )
    return usual, first


def order_table(plan):
    table = np.zeros((plan.out_rows, plan.out_rows))
    for i in range(plan.pairs):
        for neg in range(2):
            for k in range(plan.block_b):
                row = (k * 2 + neg) * plan.pairs + i
                table[row, (i * 2 + neg) * plan.block_b + k] = 1.0
    return table


def dot(left, right):
    return jnp.dot(left, right, preferred_element_type=jnp.float32)


def lane_index(shape):
    return lax.broadcasted_iota(jnp.int32, shape, 1)


def turn_lanes(value, amount):
    amount = amount % LANES
    return value if amount == 0 else pltpu.roll(value, amount, 1)


def by_lane(pieces, sub):
    out = pieces[0]
    lane = lane_index(out.shape)
    for n in range(1, len(pieces)):
        out = jnp.where(lane >= n * sub, pieces[n], out)
    return out


def far_kernel(
    plan, depth, x_hbm, gain_hbm, w_hbm, table_hbm, out_ref, near_ref, normed_ref, x_ref, gain_ref, table_ref, w_ref, sems, w_sems
):
    wide = plan.half_wide
    other = 1 - lax.axis_index("row") // (plan.rows // 2)
    x_copy = pltpu.make_async_copy(x_hbm, x_ref, sems.at[0])
    gain_copy = pltpu.make_async_copy(gain_hbm, gain_ref, sems.at[1])
    table_copy = pltpu.make_async_copy(table_hbm, table_ref, sems.at[2])
    x_copy.start()
    gain_copy.start()
    steps = plan.features // depth
    copies = []
    for n in range(steps):
        rows = pl.ds(n * depth, depth)
        far = pltpu.make_async_copy(
            w_hbm.at[rows, pl.ds(pl.multiple_of(other * wide, LANES), wide)],
            w_ref.at[rows, pl.ds(0, wide)],
            w_sems.at[0, n],
        )
        last = pltpu.make_async_copy(
            w_hbm.at[rows, pl.ds(2 * wide, GROUP)], w_ref.at[rows, pl.ds(wide, GROUP)], w_sems.at[1, n]
        )
        far.start()
        last.start()
        copies.append((far, last))
    table_copy.start()
    gain_copy.wait()
    gain = gain_ref[...].astype(jnp.float32)
    x_copy.wait()
    step = 48 if plan.local % 48 == 0 else TILE
    for start in range(0, plan.local, step):
        rows = slice(start, start + step)
        total = jnp.zeros((step, LANES), jnp.float32)
        for n in range(plan.features // LANES):
            part = x_ref[rows, n * LANES : (n + 1) * LANES].astype(jnp.float32)
            total = total + part * part
        mean = jnp.sum(total, axis=-1, keepdims=True) * (1.0 / plan.features)
        scale = lax.rsqrt(mean + norm_eps)
        for n in range(plan.features // LANES):
            columns = slice(n * LANES, (n + 1) * LANES)
            part = x_ref[rows, columns].astype(jnp.float32)
            normed_ref[rows, columns] = (part * scale * gain[n : n + 1, :]).astype(jnp.bfloat16)
    total = None
    for n in range(steps):
        for copy in copies[n]:
            copy.wait()
        rows = slice(n * depth, (n + 1) * depth)
        part = dot(normed_ref[:, rows], w_ref[rows, :])
        total = part if n == 0 else total + part
    mapped = total.astype(jnp.bfloat16)
    table_copy.wait()
    values = dot(mapped[:, wide:], table_ref[:GROUP, :GROUP])
    sub, base = plan.sub, plan.full * plan.local
    turned = [turn_lanes(values, sub * t).astype(jnp.bfloat16) for t in range(plan.rows)]
    lower = other == 0
    for dest in range(plan.rows // 2):
        for h in range(2):
            for quad in range(plan.quads):
                ends = []
                for high in range(2):
                    pieces = []
                    for inner in range(plan.rows):
                        b9 = quad * plan.rows + inner
                        if b9 < plan.half:
                            row = (h * plan.half + b9) * TILE
                            turn = (inner - dest - high * (plan.rows // 2)) % plan.rows
                            pieces.append(turned[turn][row : row + TILE, :])
                    ends.append(by_lane(pieces, sub))
                at = (h * plan.quads + quad) * TILE
                out_ref[dest, base + at : base + at + TILE, :] = jnp.where(lower, ends[0], ends[1])
                near_ref[dest, at : at + TILE, :] = jnp.where(lower, ends[1], ends[0])
    spread(plan, mapped, table_ref, out_ref)


def spread(plan, mapped, table_ref, out_ref):
    for dest in range(plan.rows // 2):
        values = dot(mapped[:, dest * 2 * GROUP : (dest + 1) * 2 * GROUP], table_ref[...])
        for f in range(plan.full):
            out_ref[dest, f * plan.local : (f + 1) * plan.local, :] = values[
                :, f * GROUP : (f + 1) * GROUP
            ].astype(jnp.bfloat16)


def near_kernel(plan, depth, normed_ref, near_ref, w_hbm, table_hbm, out_ref, table_ref, w_ref, sem, w_sems):
    wide = plan.half_wide
    mine = lax.axis_index("row") // (plan.rows // 2)
    steps = plan.features // depth
    copies = []
    for n in range(steps):
        rows = pl.ds(n * depth, depth)
        copy = pltpu.make_async_copy(
            w_hbm.at[rows, pl.ds(pl.multiple_of(mine * wide, LANES), wide)], w_ref.at[rows, :], w_sems.at[n]
        )
        copy.start()
        copies.append(copy)
    table_copy = pltpu.make_async_copy(table_hbm, table_ref, sem)
    table_copy.start()
    out_ref[:, plan.full * plan.local :, :] = near_ref[...]
    total = None
    for n in range(steps):
        copies[n].wait()
        rows = slice(n * depth, (n + 1) * depth)
        part = dot(normed_ref[:, rows], w_ref[rows, :])
        total = part if n == 0 else total + part
    table_copy.wait()
    spread(plan, total.astype(jnp.bfloat16), table_ref, out_ref)


def first_kernel(plan, *refs):
    slabs, (table_ref, out_ref, held_ref) = refs[: plan.rows], refs[plan.rows :]
    row = lax.axis_index("row")
    for s in range(plan.rows):
        held_ref[row ^ s] = slabs[s][...]
    for b9 in range(plan.half):
        quad, inner = divmod(b9, plan.rows)
        columns = []
        for f in range(plan.full):
            parts = []
            for h in range(2):
                at = f * plan.local + (h * plan.half + b9) * TILE
                parts += [held_ref[r, at : at + TILE, :] for r in range(plan.rows)]
            columns.append(jnp.concatenate(parts, axis=0))
        parts = []
        for h in range(2):
            at = plan.full * plan.local + (h * plan.quads + quad) * TILE
            parts += [held_ref[r, at : at + TILE, :] for r in range(plan.rows)]
        columns.append(jnp.concatenate(parts, axis=0))
        result = dot(table_ref[b9], jnp.concatenate(columns, axis=1))
        for f in range(plan.full):
            at = (f * plan.half + b9) * TILE
            piece = result[:, f * LANES : (f + 1) * LANES].astype(jnp.bfloat16)
            for c in range(plan.cols):
                out_ref[c, at : at + TILE, :] = piece[c * TILE : (c + 1) * TILE, :]
        tail = result[:, plan.full * LANES :]
        packed = tail if inner == 0 else jnp.where(lane_index(tail.shape) >= inner * plan.sub, tail, packed)
        if inner == plan.rows - 1 or b9 == plan.half - 1:
            at = (plan.full * plan.half + quad) * TILE
            piece = packed.astype(jnp.bfloat16)
            for c in range(plan.cols):
                out_ref[c, at : at + TILE, :] = piece[c * TILE : (c + 1) * TILE, :]


def second_far_kernel(plan, scaling, *refs):
    slabs = refs[: plan.cols]
    usual_ref, first_ref, out_ref, rhs_ref, held_ref = refs[plan.cols :]
    col = lax.axis_index("col")
    for s, pair in enumerate(crossing(plan.cols)):
        held_ref[col ^ by_parity(col, sources(pair))] = slabs[s][...]
    sub, quarter = plan.sub, TILE // 2
    low = lax.broadcasted_iota(jnp.int32, (TILE, LANES), 0) < quarter
    for b9 in range(plan.half):
        quad, inner = divmod(b9, plan.rows)
        places = [(f * plan.half + b9) * TILE for f in range(plan.full)]
        places.append((plan.full * plan.half + quad) * TILE)
        for p in range(plan.cols // 2):
            at = b9 * (plan.cols // 2) * TILE + p * TILE
            for n, place in enumerate(places):
                even = held_ref[2 * p, place : place + TILE, :].astype(jnp.float32)
                odd = held_ref[2 * p + 1, place : place + TILE, :].astype(jnp.float32)
                both = [
                    jnp.where(low, even, pltpu.roll(odd, quarter, 0)),
                    jnp.where(low, pltpu.roll(even, quarter, 0), odd),
                ]
                for i in range(plan.pairs):
                    value = both[i]
                    if n == plan.full:
                        value = turn_lanes(value, -inner * sub)
                    rhs_ref[i, at : at + TILE, n * LANES : (n + 1) * LANES] = value.astype(jnp.bfloat16)
    other = 1 - lax.axis_index("row") // (plan.rows // 2)
    transform(plan, scaling, other, usual_ref, first_ref, rhs_ref, out_ref)


def second_near_kernel(plan, scaling, usual_ref, first_ref, rhs_ref, out_ref):
    mine = lax.axis_index("row") // (plan.rows // 2)
    transform(plan, scaling, mine, usual_ref, first_ref, rhs_ref, out_ref)


def transform(plan, scaling, which, usual_ref, first_ref, rhs_ref, out_ref):
    row = lax.axis_index("row")
    sub = plan.sub
    wide = (plan.full + 1) * LANES
    lane = lane_index((1, wide))
    last = lane >= plan.full * LANES
    place = jnp.where(last, lane - plan.full * LANES + row * sub, lane & (LANES - 1))
    is_sine = place > GROUP // 2
    span = 2 * plan.block_b
    devices = plan.rows // 2
    size, total = devices * span, plan.rows * span
    tails = {}
    for i in range(plan.pairs):
        table = first_ref if i == 0 else usual_ref
        start = pl.multiple_of(which * size, TILE)
        rows = jnp.concatenate([table[pl.ds(start, size), :], table[pl.ds(total + start, size), :]], axis=0)
        both = dot(rows, rhs_ref[i])
        for r in range(devices):
            cosine, sine = both[r * span : (r + 1) * span, :], both[size + r * span : size + (r + 1) * span, :]
            merged = jnp.where(is_sine, sine, cosine) * scaling
            for f in range(plan.full):
                at = f * plan.out_rows + i * span
                out_ref[r, at : at + span, :] = merged[:, f * LANES : (f + 1) * LANES].astype(jnp.bfloat16)
            tails[i, r] = merged[:, plan.full * LANES :]
    for r in range(devices):
        pieces = []
        for t in range(plan.row_tiles):
            i, at = divmod(t * TILE, span)
            pieces.append(turn_lanes(tails[i, r][at : at + TILE, :], (t % plan.rows) * sub))
        for whole in range(plan.back_quads):
            at = plan.full * plan.out_rows + whole * TILE
            group = pieces[whole * plan.rows : (whole + 1) * plan.rows]
            out_ref[r, at : at + TILE, :] = by_lane(group, sub).astype(jnp.bfloat16)


def unfolded(plan, order, unfold, slabs):
    pair = [slabs[f * plan.out_rows : (f + 1) * plan.out_rows, :] for f in range(plan.full)]
    ordered = dot(order, jnp.concatenate(pair, axis=1)).astype(jnp.bfloat16)
    return dot(ordered, unfold).astype(jnp.bfloat16)


def early_kernel(plan, slab_ref, unfold_ref, order_ref, w_hbm, partial_ref, w_ref, own_ref, raw_ref, sems):
    row = lax.axis_index("row")
    each = plan.full * GROUP

    def part(s):
        return w_hbm.at[pl.ds(pl.multiple_of((row ^ s) * each, LANES), each), :]

    copies = [pltpu.make_async_copy(part(0), own_ref, sems.at[0])]
    for s in range(1, plan.rows):
        copies.append(pltpu.make_async_copy(part(s), raw_ref.at[pl.ds((s - 1) * each, each), :], sems.at[s]))
    copies.append(
        pltpu.make_async_copy(
            w_hbm.at[pl.ds(plan.rows * each, GROUP), :],
            raw_ref.at[pl.ds((plan.rows - 1) * each, GROUP), :],
            sems.at[plan.rows],
        )
    )
    for copy in copies:
        copy.start()
    unfold = unfold_ref[...]
    spectrum = unfolded(plan, order_ref[...], unfold, slab_ref)
    copies[0].wait()
    for n in range(plan.features // WIDE):
        columns = slice(n * WIDE, (n + 1) * WIDE)
        partial_ref[:, columns] = dot(spectrum, own_ref[:, columns])
    for s in range(1, plan.rows + 1):
        copies[s].wait()
        size = each if s < plan.rows else GROUP
        rows = slice((s - 1) * each, (s - 1) * each + size)
        for n in range(plan.features // 512):
            columns = slice(n * 512, (n + 1) * 512)
            w_ref[rows, columns] = dot(unfold[:size, :size], raw_ref[rows, columns]).astype(jnp.bfloat16)


def tail_kernel(plan, *refs):
    slabs = refs[: plan.rows]
    order_ref, partial_ref, w_ref, out_hbm, packed_ref, stage_ref, sems = refs[plan.rows :]
    row = lax.axis_index("row")
    main = plan.full * plan.out_rows
    for s in range(plan.rows):
        packed_ref[row ^ s] = slabs[s][main:, :]
    packed = [packed_ref[q].astype(jnp.float32) for q in range(plan.rows)]
    turned = [[turn_lanes(value, plan.sub * t) for t in range(plan.rows)] for value in packed]
    pieces = []
    for t in range(plan.row_tiles):
        whole, inner = divmod(t, plan.rows)
        rows = slice(whole * TILE, (whole + 1) * TILE)
        pieces.append(
            by_lane([turned[q][(q - inner) % plan.rows][rows, :] for q in range(plan.rows)], plan.sub)
        )
    parts = []
    for s in range(1, plan.rows):
        parts += [slabs[s][f * plan.out_rows : (f + 1) * plan.out_rows, :] for f in range(plan.full)]
    parts.append(jnp.concatenate(pieces, axis=0).astype(jnp.bfloat16))
    ordered = dot(order_ref[...], jnp.concatenate(parts, axis=1)).astype(jnp.bfloat16)
    group = 2 * plan.pairs
    copies = []
    for n in range(plan.features // WIDE):
        columns = slice(n * WIDE, (n + 1) * WIDE)
        result = (partial_ref[:, columns] + dot(ordered, w_ref[:, columns])).astype(jnp.bfloat16)
        for k in range(plan.block_b):
            stage_ref[n, k] = result[k * group : (k + 1) * group, :]
        copy = pltpu.make_async_copy(stage_ref.at[n], out_hbm.at[:, :, pl.ds(n * WIDE, WIDE)], sems.at[n])
        copy.start()
        copies.append(copy)
    for copy in copies:
        copy.wait()


def estimate(flops, moved):
    return pl.CostEstimate(flops=flops, bytes_accessed=moved, transcendentals=0)


def limit(mebibytes):
    return pltpu.CompilerParams(vmem_limit_bytes=mebibytes * 2**20)


def by_parity(index, pair):
    return pair[0] + (index % 2) * (pair[1] - pair[0])


def sources(pair):
    return pair if pair[0] % 2 == 0 else pair[::-1]


def exchange(values, axis, size, pairs=None):
    here = lax.axis_index(axis)
    out = []
    for s in range(size):
        pair = pairs[s] if pairs else (s, s)
        there = here ^ by_parity(here, pair)
        if isinstance(values, tuple):
            source, index = values[2 * s // size], there % (size // 2)
        else:
            source, index = values, there
        slab = lax.dynamic_index_in_dim(source, index, 0, keepdims=False)
        if s:
            slab = lax.ppermute(slab, axis, [(n, n ^ pair[n % 2]) for n in range(size)])
        out.append(slab)
    return out


def crossing(cols):
    pairs = [(s, s) for s in range(cols)]
    return CROSS if cols == len(CROSS) else pairs


def packed(plan, tokens, norm_gain, w_in, w_out):
    half_type = jnp.bfloat16
    scaling = 1.0 / math.sqrt(plan.positions * GROUP)
    col = lax.axis_index("col")
    local, features, channels = plan.local, plan.features, plan.channels
    x = tokens.transpose(1, 0, 2).reshape(local, features)
    channel = jnp.asarray(paired(channel_table()), half_type)
    gain = norm_gain.reshape(features // LANES, LANES)
    x, gain, w_in, channel = (pltpu.with_memory_space_constraint(v, pltpu.HBM) for v in (x, gain, w_in, channel))
    depth, wide = features // STEPS, plan.half_wide
    packed_rows = 2 * plan.quads * TILE
    far, near, normed = pl.pallas_call(
        functools.partial(far_kernel, plan, depth),
        out_shape=(
            pltpu.VMEM((plan.rows // 2, plan.send_rows, LANES), half_type),
            pltpu.VMEM((plan.rows // 2, packed_rows, LANES), half_type),
            pltpu.VMEM((local, features), half_type),
        ),
        in_specs=[HBM] * 4,
        out_specs=(VMEM, VMEM, VMEM),
        scratch_shapes=[
            pltpu.VMEM((local, features), half_type),
            pltpu.VMEM((features // LANES, LANES), half_type),
            pltpu.VMEM((2 * GROUP, 2 * GROUP), half_type),
            pltpu.VMEM((features, wide + GROUP), half_type),
            pltpu.SemaphoreType.DMA((3,)),
            pltpu.SemaphoreType.DMA((2, STEPS)),
        ],
        compiler_params=pltpu.CompilerParams(vmem_limit_bytes=16 * 2**20),
        cost_estimate=estimate(local * features * channels, features * channels),
        name="far",
    )(x, gain, w_in, channel)
    close = pl.pallas_call(
        functools.partial(near_kernel, plan, depth),
        out_shape=pltpu.VMEM((plan.rows // 2, plan.send_rows, LANES), half_type),
        in_specs=[VMEM, VMEM, HBM, HBM],
        out_specs=VMEM,
        scratch_shapes=[
            pltpu.VMEM((2 * GROUP, 2 * GROUP), half_type),
            pltpu.VMEM((features, wide), half_type),
            pltpu.SemaphoreType.DMA,
            pltpu.SemaphoreType.DMA((STEPS,)),
        ],
        compiler_params=pltpu.CompilerParams(vmem_limit_bytes=8 * 2**20),
        cost_estimate=estimate(local * features * channels, features * channels),
        name="near",
    )(normed, near, w_in, channel)
    slabs = exchange((close, far), "row", plan.rows)
    first = lax.dynamic_index_in_dim(jnp.asarray(first_tables(plan), half_type), col, 0, keepdims=False)
    turned = pl.pallas_call(
        functools.partial(first_kernel, plan),
        out_shape=jax.ShapeDtypeStruct((plan.cols, plan.tiles * TILE, LANES), half_type),
        in_specs=[VMEM] * (plan.rows + 1),
        out_specs=VMEM,
        scratch_shapes=[pltpu.VMEM((plan.rows, plan.send_rows, LANES), half_type)],
        compiler_params=limit(8),
        cost_estimate=estimate(10**8, 10**6),
        name="first",
    )(*slabs, first)
    slabs = exchange(turned, "col", plan.cols, crossing(plan.cols))
    usual, special = (jnp.asarray(table, half_type) for table in second_tables(plan))
    usual, special = (table.reshape(-1, table.shape[-1]) for table in (usual, special))
    leading = jnp.where(col == 0, special, usual)
    depth = plan.half * plan.cols * 4
    slab = pltpu.VMEM((plan.rows // 2, plan.back_rows, LANES), half_type)
    rhs = pltpu.VMEM((plan.pairs, depth, (plan.full + 1) * LANES), half_type)
    back_far, rhs = pl.pallas_call(
        functools.partial(second_far_kernel, plan, scaling),
        out_shape=(slab, rhs),
        in_specs=[VMEM] * (plan.cols + 2),
        out_specs=(VMEM, VMEM),
        scratch_shapes=[pltpu.VMEM((plan.cols, plan.tiles * TILE, LANES), half_type)],
        compiler_params=limit(12),
        cost_estimate=estimate(3 * 10**8, 10**6),
        name="second_far",
    )(*slabs, usual, leading)
    back_near = pl.pallas_call(
        functools.partial(second_near_kernel, plan, scaling),
        out_shape=slab,
        in_specs=[VMEM] * 3,
        out_specs=VMEM,
        compiler_params=limit(12),
        cost_estimate=estimate(3 * 10**8, 10**6),
        name="second_near",
    )(usual, leading, rhs)
    slabs = exchange((back_near, back_far), "row", plan.rows)
    unfold = jnp.asarray(paired(unfold_table()), half_type)
    order = jnp.asarray(order_table(plan), half_type)
    main, each = plan.full * plan.out_rows, plan.full * GROUP
    cost = estimate(local * features * channels, features * channels)
    partial, w_rest = pl.pallas_call(
        functools.partial(early_kernel, plan),
        out_shape=(
            pltpu.VMEM((plan.out_rows, features), jnp.float32),
            pltpu.VMEM((channels - each, features), half_type),
        ),
        in_specs=[VMEM] * 3 + [HBM],
        out_specs=(VMEM, VMEM),
        scratch_shapes=[
            pltpu.VMEM((each, features), half_type),
            pltpu.VMEM((channels - each, features), half_type),
            pltpu.SemaphoreType.DMA((plan.rows + 1,)),
        ],
        compiler_params=limit(14),
        cost_estimate=cost,
        name="early",
    )(slabs[0], unfold, order, pltpu.with_memory_space_constraint(w_out, pltpu.HBM))
    return pl.pallas_call(
        functools.partial(tail_kernel, plan),
        out_shape=jax.ShapeDtypeStruct((plan.block_b, 2 * plan.pairs, features), half_type),
        in_specs=[VMEM] * (plan.rows + 3),
        out_specs=HBM,
        scratch_shapes=[
            pltpu.VMEM((plan.rows, plan.back_rows - main, LANES), half_type),
            pltpu.VMEM((features // WIDE, plan.block_b, 2 * plan.pairs, WIDE), half_type),
            pltpu.SemaphoreType.DMA((features // WIDE,)),
        ],
        compiler_params=limit(12),
        cost_estimate=cost,
        name="tail",
    )(*slabs, order, partial, w_rest)


def shards(tokens, norm_gain, w_in, w_out):
    rows_first, rows_second, features = tokens.shape
    plan = Plan(
        lax.axis_size("row"), lax.axis_size("col"), rows_first, rows_second, features, w_in.shape[1]
    )
    if plan.fits():
        return packed(plan, tokens, norm_gain, w_in, w_out)
    return general(tokens, norm_gain, w_in, w_out)


def solution(mesh):
    in_specs = (P("row", "col", None), P(), P(), P())
    out_specs = P("row", "col", None)

    return jax.shard_map(shards, mesh=mesh, in_specs=in_specs, out_specs=out_specs, check_vma=False)
```

```python
import functools
import math

import jax
import jax.numpy as jnp
import numpy as np
from jax import lax
from jax.experimental import pallas as pl
from jax.experimental.pallas import tpu as pltpu
from jax.sharding import PartitionSpec as P

GROUP = 128


norm_eps = 1e-06
highest = lax.Precision.HIGHEST


def tables(length):
    series = jnp.arange(length, dtype=jnp.int32)
    product = series[:, None] * series[None, :] % length
    angles = product.astype(jnp.float32) * (2.0 * math.pi / length)
    return (jnp.cos(angles), jnp.sin(angles))


def folded_order(length_first, devices):
    block = length_first // devices
    half_block = block // 2
    series = jnp.arange(length_first, dtype=jnp.int32)
    device = series // block
    inner = series % block
    lower = device * half_block + inner
    upper = length_first - device * half_block - (inner - half_block)
    upper = jnp.where((device == 0) & (inner == half_block), length_first // 2, upper)
    return jnp.where(inner < half_block, lower, upper) % length_first


def to_channels(values, row_count):
    rows_first, rows_second, channels = values.shape
    width = channels // row_count
    parted = values.reshape(rows_first, rows_second, row_count, width).transpose(2, 0, 1, 3)
    return parted.reshape(row_count * rows_first, rows_second * width)


def product(table, values):
    return jnp.dot(table, values, precision=highest)


def middle(real_part, imag_part, width):
    length_first = real_part.shape[0]
    rows_second = real_part.shape[1] // width
    col_count = lax.axis_size("col")
    length_second = rows_second * col_count
    positions = length_first * length_second
    frequency = folded_order(length_first, col_count)
    series = jnp.arange(length_first, dtype=jnp.int32)
    first_angle = (frequency[:, None] * series[None, :] % length_first).astype(jnp.float32)
    first_angle = first_angle * (2.0 * math.pi / length_first)
    first_cos = jnp.cos(first_angle)
    first_sin = jnp.sin(first_angle)
    first_real = product(first_cos, real_part)
    first_imag = -product(first_sin, real_part)
    first_real = first_real + product(first_sin, imag_part)
    first_imag = first_imag + product(first_cos, imag_part)
    first_real = first_real.reshape(length_first, rows_second, width)
    first_imag = first_imag.reshape(length_first, rows_second, width)
    second_index = lax.axis_index("col") * rows_second + jnp.arange(rows_second, dtype=jnp.int32)
    twiddle_angle = (frequency[:, None] * second_index[None, :] % positions).astype(jnp.float32)
    twiddle_angle = twiddle_angle * (2.0 * math.pi / positions)
    twiddle_cos = jnp.cos(twiddle_angle)[:, :, None]
    twiddle_sin = jnp.sin(twiddle_angle)[:, :, None]
    turned_real = first_real * twiddle_cos + first_imag * twiddle_sin
    turned_imag = first_imag * twiddle_cos - first_real * twiddle_sin
    turned = jnp.stack([turned_real, turned_imag]).transpose(0, 2, 1, 3)
    turned = turned.reshape(2, rows_second, length_first * width)
    exchanged = lax.all_to_all(
        turned.astype(jnp.bfloat16), "col", split_axis=2, concat_axis=1, tiled=True
    ).astype(turned.dtype)
    second_cos, second_sin = tables(length_second)
    block = length_first // col_count
    out_shape = (length_second, block, width)
    out_real = (product(second_cos, exchanged[0]) + product(second_sin, exchanged[1])).reshape(
        out_shape
    )
    return out_real


def general(tokens, norm_gain, w_in, w_out):
    rows_first, rows_second, features = tokens.shape
    row_count = lax.axis_size("row")
    length_first = rows_first * row_count
    length_second = rows_second * lax.axis_size("col")
    channels = w_in.shape[1]
    width = channels // row_count
    groups = channels // GROUP
    scaling = 1.0 / math.sqrt(length_first * length_second * GROUP)
    floats = tokens.astype(jnp.float32)
    normed = (
        floats
        * lax.rsqrt(jnp.mean(floats * floats, axis=-1, keepdims=True) + norm_eps)
        * norm_gain.astype(jnp.float32)
    ).astype(jnp.bfloat16)
    mapped = jnp.dot(normed.reshape(-1, features), w_in, preferred_element_type=jnp.float32)
    mapped = mapped.astype(jnp.bfloat16).reshape(rows_first, rows_second, channels)
    channel_cos, channel_sin = tables(GROUP)
    grouped = mapped.astype(jnp.float32).reshape(rows_first, rows_second, groups, GROUP)
    spec_real = jnp.einsum("abgj,jm->abgm", grouped, channel_cos, precision=highest)
    spec_imag = -jnp.einsum("abgj,jm->abgm", grouped, channel_sin, precision=highest)
    stacked = jnp.stack(
        [
            to_channels(spec_real.reshape(rows_first, rows_second, channels), row_count),
            to_channels(spec_imag.reshape(rows_first, rows_second, channels), row_count),
        ]
    )
    arrived = lax.all_to_all(
        stacked.astype(jnp.bfloat16), "row", split_axis=1, concat_axis=1, tiled=True
    ).astype(stacked.dtype)
    result = middle(arrived[0], arrived[1], width)
    spectrum = (result * scaling).astype(jnp.bfloat16)
    returned = lax.all_to_all(spectrum, "row", split_axis=0, concat_axis=2, tiled=True)
    mixed = jnp.dot(returned.reshape(-1, channels), w_out, preferred_element_type=jnp.float32)
    return mixed.astype(jnp.bfloat16).reshape(returned.shape[0], returned.shape[1], features)


LANES = 128
TILE = 8
STEPS = 1
WIDE = 256
RELAYED = ((0, 0), (1, 1), (2, 4), (5, 3), (4, 2), (3, 5), (6, 6), (7, 7))
VMEM = pl.BlockSpec(memory_space=pltpu.VMEM)
HBM = pl.BlockSpec(memory_space=pltpu.HBM)


class Plan:
    def __init__(self, rows, cols, rows_first, rows_second, features, channels):
        self.rows, self.cols = rows, cols
        self.rows_first, self.rows_second = rows_first, rows_second
        self.features, self.channels = features, channels
        self.length_first = rows_first * rows
        self.length_second = rows_second * cols
        self.positions = self.length_first * self.length_second
        self.groups = channels // GROUP
        self.full = self.groups // rows
        self.sub = GROUP // rows
        self.half = rows_second // 2
        self.quads = -(-self.half // rows)
        self.tiles = self.full * self.half + self.quads
        self.local = rows_first * rows_second
        self.half_wide = rows // 2 * self.full * GROUP
        self.send_rows = self.full * self.local + 2 * self.quads * TILE
        self.pairs = self.length_first // cols // 2
        self.block_b = self.length_second // rows
        self.out_rows = self.block_b * 2 * self.pairs
        self.row_tiles = self.out_rows // TILE
        self.back_quads = -(-self.row_tiles // rows)
        self.back_rows = self.full * self.out_rows + self.back_quads * TILE

    def fits(self):
        return (
            GROUP == LANES
            and self.rows & (self.rows - 1) == 0
            and self.cols & (self.cols - 1) == 0
            and 1 < self.rows <= 8
            and self.cols > 1
            and self.rows_first == TILE
            and self.rows_second % 2 == 0
            and self.channels % GROUP == 0
            and self.groups % self.rows == 1
            and self.full == 2
            and self.length_first == 4 * self.cols
            and self.length_second % self.rows == 0
            and 2 * self.block_b % TILE == 0
            and self.features % 512 == 0
        )


def channel_table():
    j = np.arange(GROUP)[:, None]
    u = np.arange(GROUP)[None, :]
    half = GROUP // 2
    m = np.where(u <= half, u, u - half)
    angle = 2.0 * np.pi * (j * m % GROUP) / GROUP
    return np.where(u <= half, np.cos(angle), np.sin(angle))


def unfold_table():
    half = GROUP // 2
    table = np.zeros((GROUP, GROUP))
    for m in range(GROUP):
        near = m if m <= half else GROUP - m
        table[near, m] = 1.0
        if 0 < near < half:
            table[half + near, m] = -1.0 if m < half else 1.0
    return table


def paired(table):
    zero = np.zeros_like(table)
    return np.block([[table, zero], [zero, table]])


def first_tables(plan):
    a = np.arange(plan.length_first)
    out = np.zeros((plan.cols, plan.half, plan.cols, plan.pairs, 2, 2, 2, plan.length_first))
    for col in range(plan.cols):
        for b9 in range(plan.half):
            for h in range(2):
                b = col * plan.rows_second + h * plan.half + b9
                for c in range(plan.cols):
                    for i in range(plan.pairs):
                        k = c * plan.pairs + i
                        if k == 0:
                            out[col, b9, c, i, h, 0, h] = 1.0
                            out[col, b9, c, i, h, 1, h] = np.where(a % 2 == 0, 1.0, -1.0)
                        else:
                            phase = (a * plan.length_second + b) * k % plan.positions
                            angle = 2.0 * np.pi * phase / plan.positions
                            out[col, b9, c, i, h, 0, h] = np.cos(angle)
                            out[col, b9, c, i, h, 1, h] = -np.sin(angle)
    size = 2 * plan.length_first
    return out.reshape(plan.cols, plan.half, size, size)


def second_tables(plan):
    length = plan.length_second
    b9 = np.arange(plan.half)[:, None, None]
    c = np.arange(plan.cols)[None, :, None]
    h = np.arange(2)[None, None, :]
    b = (c * plan.rows_second + h * plan.half + b9).reshape(-1)
    k = np.arange(length)
    angle = 2.0 * np.pi * (k[:, None] * b[None, :] % length) / length
    cos, sin = np.cos(angle), np.sin(angle)
    cosine = np.stack([cos, sin], axis=-1)
    sine = np.stack([sin, -cos], axis=-1)

    def arrange(plus, minus):
        both = np.stack([plus, minus]).reshape(2, plan.rows, plan.block_b, -1)
        return both.transpose(1, 0, 2, 3).reshape(2 * length, -1)

    usual = np.stack([arrange(cosine, cosine[::-1]), arrange(sine, -sine[::-1])])
    turn = 2.0 * np.pi * ((plan.length_first // 2) * b % plan.positions) / plan.positions
    late = angle + turn[None, :]
    zero = np.zeros_like(cos)
    first = np.stack(
        [
            arrange(np.stack([cos, zero], -1), np.stack([zero, np.cos(late)], -1)),
            arrange(np.stack([sin, zero], -1), np.stack([zero, np.sin(late)], -1)),
        ]
    )
    return usual, first


def order_table(plan):
    table = np.zeros((plan.out_rows, plan.out_rows))
    for i in range(plan.pairs):
        for neg in range(2):
            for k in range(plan.block_b):
                row = (k * 2 + neg) * plan.pairs + i
                table[row, (i * 2 + neg) * plan.block_b + k] = 1.0
    return table


def dot(left, right):
    return jnp.dot(left, right, preferred_element_type=jnp.float32)


def lane_index(shape):
    return lax.broadcasted_iota(jnp.int32, shape, 1)


def turn_lanes(value, amount):
    amount = amount % LANES
    return value if amount == 0 else pltpu.roll(value, amount, 1)


def by_lane(pieces, sub):
    out = pieces[0]
    lane = lane_index(out.shape)
    for n in range(1, len(pieces)):
        out = jnp.where(lane >= n * sub, pieces[n], out)
    return out


def far_kernel(
    plan, depth, x_hbm, gain_hbm, w_hbm, table_hbm, out_ref, near_ref, normed_ref, x_ref, gain_ref, table_ref, w_ref, sems, w_sems
):
    wide = plan.half_wide
    other = 1 - lax.axis_index("row") // (plan.rows // 2)
    x_copy = pltpu.make_async_copy(x_hbm, x_ref, sems.at[0])
    gain_copy = pltpu.make_async_copy(gain_hbm, gain_ref, sems.at[1])
    table_copy = pltpu.make_async_copy(table_hbm, table_ref, sems.at[2])
    x_copy.start()
    gain_copy.start()
    steps = plan.features // depth
    copies = []
    for n in range(steps):
        rows = pl.ds(n * depth, depth)
        far = pltpu.make_async_copy(
            w_hbm.at[rows, pl.ds(pl.multiple_of(other * wide, LANES), wide)],
            w_ref.at[rows, pl.ds(0, wide)],
            w_sems.at[0, n],
        )
        last = pltpu.make_async_copy(
            w_hbm.at[rows, pl.ds(2 * wide, GROUP)], w_ref.at[rows, pl.ds(wide, GROUP)], w_sems.at[1, n]
        )
        far.start()
        last.start()
        copies.append((far, last))
    table_copy.start()
    gain_copy.wait()
    gain = gain_ref[...].astype(jnp.float32)
    x_copy.wait()
    step = 48 if plan.local % 48 == 0 else TILE
    for start in range(0, plan.local, step):
        rows = slice(start, start + step)
        total = jnp.zeros((step, LANES), jnp.float32)
        for n in range(plan.features // LANES):
            part = x_ref[rows, n * LANES : (n + 1) * LANES].astype(jnp.float32)
            total = total + part * part
        mean = jnp.sum(total, axis=-1, keepdims=True) * (1.0 / plan.features)
        scale = lax.rsqrt(mean + norm_eps)
        for n in range(plan.features // LANES):
            columns = slice(n * LANES, (n + 1) * LANES)
            part = x_ref[rows, columns].astype(jnp.float32)
            normed_ref[rows, columns] = (part * scale * gain[n : n + 1, :]).astype(jnp.bfloat16)
    total = None
    for n in range(steps):
        for copy in copies[n]:
            copy.wait()
        rows = slice(n * depth, (n + 1) * depth)
        part = dot(normed_ref[:, rows], w_ref[rows, :])
        total = part if n == 0 else total + part
    mapped = total.astype(jnp.bfloat16)
    table_copy.wait()
    values = dot(mapped[:, wide:], table_ref[:GROUP, :GROUP])
    sub, base = plan.sub, plan.full * plan.local
    turned = [turn_lanes(values, sub * t).astype(jnp.bfloat16) for t in range(plan.rows)]
    lower = other == 0
    for dest in range(plan.rows // 2):
        for h in range(2):
            for quad in range(plan.quads):
                ends = []
                for high in range(2):
                    pieces = []
                    for inner in range(plan.rows):
                        b9 = quad * plan.rows + inner
                        if b9 < plan.half:
                            row = (h * plan.half + b9) * TILE
                            turn = (inner - dest - high * (plan.rows // 2)) % plan.rows
                            pieces.append(turned[turn][row : row + TILE, :])
                    ends.append(by_lane(pieces, sub))
                at = (h * plan.quads + quad) * TILE
                out_ref[dest, base + at : base + at + TILE, :] = jnp.where(lower, ends[0], ends[1])
                near_ref[dest, at : at + TILE, :] = jnp.where(lower, ends[1], ends[0])
    spread(plan, mapped, table_ref, out_ref)


def spread(plan, mapped, table_ref, out_ref):
    for dest in range(plan.rows // 2):
        values = dot(mapped[:, dest * 2 * GROUP : (dest + 1) * 2 * GROUP], table_ref[...])
        for f in range(plan.full):
            out_ref[dest, f * plan.local : (f + 1) * plan.local, :] = values[
                :, f * GROUP : (f + 1) * GROUP
            ].astype(jnp.bfloat16)


def near_kernel(plan, depth, normed_ref, near_ref, w_hbm, table_hbm, out_ref, table_ref, w_ref, sem, w_sems):
    wide = plan.half_wide
    mine = lax.axis_index("row") // (plan.rows // 2)
    steps = plan.features // depth
    copies = []
    for n in range(steps):
        rows = pl.ds(n * depth, depth)
        copy = pltpu.make_async_copy(
            w_hbm.at[rows, pl.ds(pl.multiple_of(mine * wide, LANES), wide)], w_ref.at[rows, :], w_sems.at[n]
        )
        copy.start()
        copies.append(copy)
    table_copy = pltpu.make_async_copy(table_hbm, table_ref, sem)
    table_copy.start()
    out_ref[:, plan.full * plan.local :, :] = near_ref[...]
    total = None
    for n in range(steps):
        copies[n].wait()
        rows = slice(n * depth, (n + 1) * depth)
        part = dot(normed_ref[:, rows], w_ref[rows, :])
        total = part if n == 0 else total + part
    table_copy.wait()
    spread(plan, total.astype(jnp.bfloat16), table_ref, out_ref)


def first_kernel(plan, *refs):
    slabs, (table_ref, out_ref, held_ref) = refs[: plan.rows], refs[plan.rows :]
    row = lax.axis_index("row")
    for s in range(plan.rows):
        held_ref[row ^ s] = slabs[s][...]
    for b9 in range(plan.half):
        quad, inner = divmod(b9, plan.rows)
        columns = []
        for f in range(plan.full):
            parts = []
            for h in range(2):
                at = f * plan.local + (h * plan.half + b9) * TILE
                parts += [held_ref[r, at : at + TILE, :] for r in range(plan.rows)]
            columns.append(jnp.concatenate(parts, axis=0))
        parts = []
        for h in range(2):
            at = plan.full * plan.local + (h * plan.quads + quad) * TILE
            parts += [held_ref[r, at : at + TILE, :] for r in range(plan.rows)]
        columns.append(jnp.concatenate(parts, axis=0))
        result = dot(table_ref[b9], jnp.concatenate(columns, axis=1))
        for f in range(plan.full):
            at = (f * plan.half + b9) * TILE
            piece = result[:, f * LANES : (f + 1) * LANES].astype(jnp.bfloat16)
            for c in range(plan.cols):
                out_ref[c, at : at + TILE, :] = piece[c * TILE : (c + 1) * TILE, :]
        tail = result[:, plan.full * LANES :]
        packed = tail if inner == 0 else jnp.where(lane_index(tail.shape) >= inner * plan.sub, tail, packed)
        if inner == plan.rows - 1 or b9 == plan.half - 1:
            at = (plan.full * plan.half + quad) * TILE
            piece = packed.astype(jnp.bfloat16)
            for c in range(plan.cols):
                out_ref[c, at : at + TILE, :] = piece[c * TILE : (c + 1) * TILE, :]


def second_far_kernel(plan, scaling, *refs):
    slabs = refs[: plan.cols]
    usual_ref, first_ref, out_ref, rhs_ref, held_ref = refs[plan.cols :]
    col = lax.axis_index("col")
    for s, pair in enumerate(crossing(plan.cols)):
        held_ref[col ^ by_parity(col, pair)] = slabs[s][: plan.tiles * TILE, :]
    sub, quarter = plan.sub, TILE // 2
    low = lax.broadcasted_iota(jnp.int32, (TILE, LANES), 0) < quarter
    for b9 in range(plan.half):
        quad, inner = divmod(b9, plan.rows)
        places = [(f * plan.half + b9) * TILE for f in range(plan.full)]
        places.append((plan.full * plan.half + quad) * TILE)
        for p in range(plan.cols // 2):
            at = b9 * (plan.cols // 2) * TILE + p * TILE
            for n, place in enumerate(places):
                even = held_ref[2 * p, place : place + TILE, :].astype(jnp.float32)
                odd = held_ref[2 * p + 1, place : place + TILE, :].astype(jnp.float32)
                both = [
                    jnp.where(low, even, pltpu.roll(odd, quarter, 0)),
                    jnp.where(low, pltpu.roll(even, quarter, 0), odd),
                ]
                for i in range(plan.pairs):
                    value = both[i]
                    if n == plan.full:
                        value = turn_lanes(value, -inner * sub)
                    rhs_ref[i, at : at + TILE, n * LANES : (n + 1) * LANES] = value.astype(jnp.bfloat16)
    other = 1 - lax.axis_index("row") // (plan.rows // 2)
    transform(plan, scaling, other, usual_ref, first_ref, rhs_ref, out_ref)


def second_near_kernel(plan, scaling, usual_ref, first_ref, rhs_ref, out_ref):
    mine = lax.axis_index("row") // (plan.rows // 2)
    transform(plan, scaling, mine, usual_ref, first_ref, rhs_ref, out_ref)


def transform(plan, scaling, which, usual_ref, first_ref, rhs_ref, out_ref):
    row = lax.axis_index("row")
    sub = plan.sub
    wide = (plan.full + 1) * LANES
    lane = lane_index((1, wide))
    last = lane >= plan.full * LANES
    place = jnp.where(last, lane - plan.full * LANES + row * sub, lane & (LANES - 1))
    is_sine = place > GROUP // 2
    span = 2 * plan.block_b
    devices = plan.rows // 2
    size, total = devices * span, plan.rows * span
    tails = {}
    for i in range(plan.pairs):
        table = first_ref if i == 0 else usual_ref
        start = pl.multiple_of(which * size, TILE)
        rows = jnp.concatenate([table[pl.ds(start, size), :], table[pl.ds(total + start, size), :]], axis=0)
        both = dot(rows, rhs_ref[i])
        for r in range(devices):
            cosine, sine = both[r * span : (r + 1) * span, :], both[size + r * span : size + (r + 1) * span, :]
            merged = jnp.where(is_sine, sine, cosine) * scaling
            for f in range(plan.full):
                at = f * plan.out_rows + i * span
                out_ref[r, at : at + span, :] = merged[:, f * LANES : (f + 1) * LANES].astype(jnp.bfloat16)
            tails[i, r] = merged[:, plan.full * LANES :]
    for r in range(devices):
        pieces = []
        for t in range(plan.row_tiles):
            i, at = divmod(t * TILE, span)
            pieces.append(turn_lanes(tails[i, r][at : at + TILE, :], (t % plan.rows) * sub))
        for whole in range(plan.back_quads):
            at = plan.full * plan.out_rows + whole * TILE
            group = pieces[whole * plan.rows : (whole + 1) * plan.rows]
            out_ref[r, at : at + TILE, :] = by_lane(group, sub).astype(jnp.bfloat16)


def unfolded(plan, order, unfold, slabs):
    pair = [slabs[f * plan.out_rows : (f + 1) * plan.out_rows, :] for f in range(plan.full)]
    ordered = dot(order, jnp.concatenate(pair, axis=1)).astype(jnp.bfloat16)
    return dot(ordered, unfold).astype(jnp.bfloat16)


def early_kernel(plan, slab_ref, unfold_ref, order_ref, w_hbm, partial_ref, w_ref, own_ref, raw_ref, sems):
    row = lax.axis_index("row")
    each = plan.full * GROUP

    def part(s):
        return w_hbm.at[pl.ds(pl.multiple_of((row ^ s) * each, LANES), each), :]

    copies = [pltpu.make_async_copy(part(0), own_ref, sems.at[0])]
    for s in range(1, plan.rows):
        copies.append(pltpu.make_async_copy(part(s), raw_ref.at[pl.ds((s - 1) * each, each), :], sems.at[s]))
    copies.append(
        pltpu.make_async_copy(
            w_hbm.at[pl.ds(plan.rows * each, GROUP), :],
            raw_ref.at[pl.ds((plan.rows - 1) * each, GROUP), :],
            sems.at[plan.rows],
        )
    )
    for copy in copies:
        copy.start()
    unfold = unfold_ref[...]
    spectrum = unfolded(plan, order_ref[...], unfold, slab_ref)
    copies[0].wait()
    for n in range(plan.features // WIDE):
        columns = slice(n * WIDE, (n + 1) * WIDE)
        partial_ref[:, columns] = dot(spectrum, own_ref[:, columns])
    for s in range(1, plan.rows + 1):
        copies[s].wait()
        size = each if s < plan.rows else GROUP
        rows = slice((s - 1) * each, (s - 1) * each + size)
        for n in range(plan.features // 512):
            columns = slice(n * 512, (n + 1) * 512)
            w_ref[rows, columns] = dot(unfold[:size, :size], raw_ref[rows, columns]).astype(jnp.bfloat16)


def tail_kernel(plan, *refs):
    slabs = refs[: plan.rows]
    order_ref, partial_ref, w_ref, out_hbm, packed_ref, stage_ref, sems = refs[plan.rows :]
    row = lax.axis_index("row")
    main = plan.full * plan.out_rows
    for s in range(plan.rows):
        packed_ref[row ^ s] = slabs[s][main:, :]
    packed = [packed_ref[q].astype(jnp.float32) for q in range(plan.rows)]
    turned = [[turn_lanes(value, plan.sub * t) for t in range(plan.rows)] for value in packed]
    pieces = []
    for t in range(plan.row_tiles):
        whole, inner = divmod(t, plan.rows)
        rows = slice(whole * TILE, (whole + 1) * TILE)
        pieces.append(
            by_lane([turned[q][(q - inner) % plan.rows][rows, :] for q in range(plan.rows)], plan.sub)
        )
    parts = []
    for s in range(1, plan.rows):
        parts += [slabs[s][f * plan.out_rows : (f + 1) * plan.out_rows, :] for f in range(plan.full)]
    parts.append(jnp.concatenate(pieces, axis=0).astype(jnp.bfloat16))
    ordered = dot(order_ref[...], jnp.concatenate(parts, axis=1)).astype(jnp.bfloat16)
    group = 2 * plan.pairs
    copies = []
    for n in range(plan.features // WIDE):
        columns = slice(n * WIDE, (n + 1) * WIDE)
        result = (partial_ref[:, columns] + dot(ordered, w_ref[:, columns])).astype(jnp.bfloat16)
        for k in range(plan.block_b):
            stage_ref[n, k] = result[k * group : (k + 1) * group, :]
        copy = pltpu.make_async_copy(stage_ref.at[n], out_hbm.at[:, :, pl.ds(n * WIDE, WIDE)], sems.at[n])
        copy.start()
        copies.append(copy)
    for copy in copies:
        copy.wait()


def estimate(flops, moved):
    return pl.CostEstimate(flops=flops, bytes_accessed=moved, transcendentals=0)


def limit(mebibytes):
    return pltpu.CompilerParams(vmem_limit_bytes=mebibytes * 2**20)


def by_parity(index, pair):
    return pair[0] + (index % 2) * (pair[1] - pair[0])


def exchange(values, axis, size):
    here = lax.axis_index(axis)
    out = []
    for s in range(size):
        there = here ^ s
        if isinstance(values, tuple):
            source, index = values[2 * s // size], there % (size // 2)
        else:
            source, index = values, there
        slab = lax.dynamic_index_in_dim(source, index, 0, keepdims=False)
        if s:
            slab = lax.ppermute(slab, axis, [(n, n ^ s) for n in range(size)])
        out.append(slab)
    return out


def crossing(cols):
    if cols == len(RELAYED):
        return RELAYED
    return tuple((s, s) for s in range(cols))


def cross(values, cols):
    if cols != len(RELAYED):
        return exchange(values, "col", cols)
    here = lax.axis_index("col")

    def slab(pair, flip=0):
        return lax.dynamic_index_in_dim(values, here ^ by_parity(here, pair) ^ flip, 0, keepdims=False)

    def send(value, pair):
        return lax.ppermute(value, "col", [(n, n ^ pair[n % 2]) for n in range(cols)])

    def both(pair):
        return jnp.concatenate([slab(pair), slab(pair, 1)], axis=0)

    rows = values.shape[1]
    diagonal = send(both((6, 6)), (6, 6))
    beside = send(both((4, 2)), (4, 2))
    crossed = send(slab((3, 5)), (3, 5))
    straight = send(slab((2, 4)), (2, 4))
    sibling = send(slab((1, 1)), (1, 1))
    diagonal_other = send(diagonal[rows:], (1, 1))
    beside_other = send(beside[rows:], (1, 1))
    return [slab((0, 0)), sibling, straight, crossed, beside, beside_other, diagonal, diagonal_other]


def packed(plan, tokens, norm_gain, w_in, w_out):
    half_type = jnp.bfloat16
    scaling = 1.0 / math.sqrt(plan.positions * GROUP)
    col = lax.axis_index("col")
    local, features, channels = plan.local, plan.features, plan.channels
    x = tokens.transpose(1, 0, 2).reshape(local, features)
    channel = jnp.asarray(paired(channel_table()), half_type)
    gain = norm_gain.reshape(features // LANES, LANES)
    x, gain, w_in, channel = (pltpu.with_memory_space_constraint(v, pltpu.HBM) for v in (x, gain, w_in, channel))
    depth, wide = features // STEPS, plan.half_wide
    packed_rows = 2 * plan.quads * TILE
    far, near, normed = pl.pallas_call(
        functools.partial(far_kernel, plan, depth),
        out_shape=(
            pltpu.VMEM((plan.rows // 2, plan.send_rows, LANES), half_type),
            pltpu.VMEM((plan.rows // 2, packed_rows, LANES), half_type),
            pltpu.VMEM((local, features), half_type),
        ),
        in_specs=[HBM] * 4,
        out_specs=(VMEM, VMEM, VMEM),
        scratch_shapes=[
            pltpu.VMEM((local, features), half_type),
            pltpu.VMEM((features // LANES, LANES), half_type),
            pltpu.VMEM((2 * GROUP, 2 * GROUP), half_type),
            pltpu.VMEM((features, wide + GROUP), half_type),
            pltpu.SemaphoreType.DMA((3,)),
            pltpu.SemaphoreType.DMA((2, STEPS)),
        ],
        compiler_params=pltpu.CompilerParams(vmem_limit_bytes=16 * 2**20),
        cost_estimate=estimate(local * features * channels, features * channels),
        name="far",
    )(x, gain, w_in, channel)
    close = pl.pallas_call(
        functools.partial(near_kernel, plan, depth),
        out_shape=pltpu.VMEM((plan.rows // 2, plan.send_rows, LANES), half_type),
        in_specs=[VMEM, VMEM, HBM, HBM],
        out_specs=VMEM,
        scratch_shapes=[
            pltpu.VMEM((2 * GROUP, 2 * GROUP), half_type),
            pltpu.VMEM((features, wide), half_type),
            pltpu.SemaphoreType.DMA,
            pltpu.SemaphoreType.DMA((STEPS,)),
        ],
        compiler_params=pltpu.CompilerParams(vmem_limit_bytes=8 * 2**20),
        cost_estimate=estimate(local * features * channels, features * channels),
        name="near",
    )(normed, near, w_in, channel)
    slabs = exchange((close, far), "row", plan.rows)
    first = lax.dynamic_index_in_dim(jnp.asarray(first_tables(plan), half_type), col, 0, keepdims=False)
    turned = pl.pallas_call(
        functools.partial(first_kernel, plan),
        out_shape=jax.ShapeDtypeStruct((plan.cols, plan.tiles * TILE, LANES), half_type),
        in_specs=[VMEM] * (plan.rows + 1),
        out_specs=VMEM,
        scratch_shapes=[pltpu.VMEM((plan.rows, plan.send_rows, LANES), half_type)],
        compiler_params=limit(8),
        cost_estimate=estimate(10**8, 10**6),
        name="first",
    )(*slabs, first)
    slabs = cross(turned, plan.cols)
    usual, special = (jnp.asarray(table, half_type) for table in second_tables(plan))
    usual, special = (table.reshape(-1, table.shape[-1]) for table in (usual, special))
    leading = jnp.where(col == 0, special, usual)
    depth = plan.half * plan.cols * 4
    slab = pltpu.VMEM((plan.rows // 2, plan.back_rows, LANES), half_type)
    rhs = pltpu.VMEM((plan.pairs, depth, (plan.full + 1) * LANES), half_type)
    back_far, rhs = pl.pallas_call(
        functools.partial(second_far_kernel, plan, scaling),
        out_shape=(slab, rhs),
        in_specs=[VMEM] * (plan.cols + 2),
        out_specs=(VMEM, VMEM),
        scratch_shapes=[pltpu.VMEM((plan.cols, plan.tiles * TILE, LANES), half_type)],
        compiler_params=limit(12),
        cost_estimate=estimate(3 * 10**8, 10**6),
        name="second_far",
    )(*slabs, usual, leading)
    back_near = pl.pallas_call(
        functools.partial(second_near_kernel, plan, scaling),
        out_shape=slab,
        in_specs=[VMEM] * 3,
        out_specs=VMEM,
        compiler_params=limit(12),
        cost_estimate=estimate(3 * 10**8, 10**6),
        name="second_near",
    )(usual, leading, rhs)
    slabs = exchange((back_near, back_far), "row", plan.rows)
    unfold = jnp.asarray(paired(unfold_table()), half_type)
    order = jnp.asarray(order_table(plan), half_type)
    main, each = plan.full * plan.out_rows, plan.full * GROUP
    cost = estimate(local * features * channels, features * channels)
    partial, w_rest = pl.pallas_call(
        functools.partial(early_kernel, plan),
        out_shape=(
            pltpu.VMEM((plan.out_rows, features), jnp.float32),
            pltpu.VMEM((channels - each, features), half_type),
        ),
        in_specs=[VMEM] * 3 + [HBM],
        out_specs=(VMEM, VMEM),
        scratch_shapes=[
            pltpu.VMEM((each, features), half_type),
            pltpu.VMEM((channels - each, features), half_type),
            pltpu.SemaphoreType.DMA((plan.rows + 1,)),
        ],
        compiler_params=limit(14),
        cost_estimate=cost,
        name="early",
    )(slabs[0], unfold, order, pltpu.with_memory_space_constraint(w_out, pltpu.HBM))
    return pl.pallas_call(
        functools.partial(tail_kernel, plan),
        out_shape=jax.ShapeDtypeStruct((plan.block_b, 2 * plan.pairs, features), half_type),
        in_specs=[VMEM] * (plan.rows + 3),
        out_specs=HBM,
        scratch_shapes=[
            pltpu.VMEM((plan.rows, plan.back_rows - main, LANES), half_type),
            pltpu.VMEM((features // WIDE, plan.block_b, 2 * plan.pairs, WIDE), half_type),
            pltpu.SemaphoreType.DMA((features // WIDE,)),
        ],
        compiler_params=limit(12),
        cost_estimate=cost,
        name="tail",
    )(*slabs, order, partial, w_rest)


def shards(tokens, norm_gain, w_in, w_out):
    rows_first, rows_second, features = tokens.shape
    plan = Plan(
        lax.axis_size("row"), lax.axis_size("col"), rows_first, rows_second, features, w_in.shape[1]
    )
    if plan.fits():
        return packed(plan, tokens, norm_gain, w_in, w_out)
    return general(tokens, norm_gain, w_in, w_out)


def solution(mesh):
    in_specs = (P("row", "col", None), P(), P(), P())
    out_specs = P("row", "col", None)

    return jax.shard_map(shards, mesh=mesh, in_specs=in_specs, out_specs=out_specs, check_vma=False)
```

```python
import functools
import math

import jax
import jax.numpy as jnp
import numpy as np
from jax import lax
from jax.experimental import pallas as pl
from jax.experimental.pallas import tpu as pltpu
from jax.sharding import PartitionSpec as P

GROUP = 128


norm_eps = 1e-06
highest = lax.Precision.HIGHEST


def tables(length):
    series = jnp.arange(length, dtype=jnp.int32)
    product = series[:, None] * series[None, :] % length
    angles = product.astype(jnp.float32) * (2.0 * math.pi / length)
    return (jnp.cos(angles), jnp.sin(angles))


def folded_order(length_first, devices):
    block = length_first // devices
    half_block = block // 2
    series = jnp.arange(length_first, dtype=jnp.int32)
    device = series // block
    inner = series % block
    lower = device * half_block + inner
    upper = length_first - device * half_block - (inner - half_block)
    upper = jnp.where((device == 0) & (inner == half_block), length_first // 2, upper)
    return jnp.where(inner < half_block, lower, upper) % length_first


def to_channels(values, row_count):
    rows_first, rows_second, channels = values.shape
    width = channels // row_count
    parted = values.reshape(rows_first, rows_second, row_count, width).transpose(2, 0, 1, 3)
    return parted.reshape(row_count * rows_first, rows_second * width)


def product(table, values):
    return jnp.dot(table, values, precision=highest)


def middle(real_part, imag_part, width):
    length_first = real_part.shape[0]
    rows_second = real_part.shape[1] // width
    col_count = lax.axis_size("col")
    length_second = rows_second * col_count
    positions = length_first * length_second
    frequency = folded_order(length_first, col_count)
    series = jnp.arange(length_first, dtype=jnp.int32)
    first_angle = (frequency[:, None] * series[None, :] % length_first).astype(jnp.float32)
    first_angle = first_angle * (2.0 * math.pi / length_first)
    first_cos = jnp.cos(first_angle)
    first_sin = jnp.sin(first_angle)
    first_real = product(first_cos, real_part)
    first_imag = -product(first_sin, real_part)
    first_real = first_real + product(first_sin, imag_part)
    first_imag = first_imag + product(first_cos, imag_part)
    first_real = first_real.reshape(length_first, rows_second, width)
    first_imag = first_imag.reshape(length_first, rows_second, width)
    second_index = lax.axis_index("col") * rows_second + jnp.arange(rows_second, dtype=jnp.int32)
    twiddle_angle = (frequency[:, None] * second_index[None, :] % positions).astype(jnp.float32)
    twiddle_angle = twiddle_angle * (2.0 * math.pi / positions)
    twiddle_cos = jnp.cos(twiddle_angle)[:, :, None]
    twiddle_sin = jnp.sin(twiddle_angle)[:, :, None]
    turned_real = first_real * twiddle_cos + first_imag * twiddle_sin
    turned_imag = first_imag * twiddle_cos - first_real * twiddle_sin
    turned = jnp.stack([turned_real, turned_imag]).transpose(0, 2, 1, 3)
    turned = turned.reshape(2, rows_second, length_first * width)
    exchanged = lax.all_to_all(
        turned.astype(jnp.bfloat16), "col", split_axis=2, concat_axis=1, tiled=True
    ).astype(turned.dtype)
    second_cos, second_sin = tables(length_second)
    block = length_first // col_count
    out_shape = (length_second, block, width)
    out_real = (product(second_cos, exchanged[0]) + product(second_sin, exchanged[1])).reshape(
        out_shape
    )
    return out_real


def general(tokens, norm_gain, w_in, w_out):
    rows_first, rows_second, features = tokens.shape
    row_count = lax.axis_size("row")
    length_first = rows_first * row_count
    length_second = rows_second * lax.axis_size("col")
    channels = w_in.shape[1]
    width = channels // row_count
    groups = channels // GROUP
    scaling = 1.0 / math.sqrt(length_first * length_second * GROUP)
    floats = tokens.astype(jnp.float32)
    normed = (
        floats
        * lax.rsqrt(jnp.mean(floats * floats, axis=-1, keepdims=True) + norm_eps)
        * norm_gain.astype(jnp.float32)
    ).astype(jnp.bfloat16)
    mapped = jnp.dot(normed.reshape(-1, features), w_in, preferred_element_type=jnp.float32)
    mapped = mapped.astype(jnp.bfloat16).reshape(rows_first, rows_second, channels)
    channel_cos, channel_sin = tables(GROUP)
    grouped = mapped.astype(jnp.float32).reshape(rows_first, rows_second, groups, GROUP)
    spec_real = jnp.einsum("abgj,jm->abgm", grouped, channel_cos, precision=highest)
    spec_imag = -jnp.einsum("abgj,jm->abgm", grouped, channel_sin, precision=highest)
    stacked = jnp.stack(
        [
            to_channels(spec_real.reshape(rows_first, rows_second, channels), row_count),
            to_channels(spec_imag.reshape(rows_first, rows_second, channels), row_count),
        ]
    )
    arrived = lax.all_to_all(
        stacked.astype(jnp.bfloat16), "row", split_axis=1, concat_axis=1, tiled=True
    ).astype(stacked.dtype)
    result = middle(arrived[0], arrived[1], width)
    spectrum = (result * scaling).astype(jnp.bfloat16)
    returned = lax.all_to_all(spectrum, "row", split_axis=0, concat_axis=2, tiled=True)
    mixed = jnp.dot(returned.reshape(-1, channels), w_out, preferred_element_type=jnp.float32)
    return mixed.astype(jnp.bfloat16).reshape(returned.shape[0], returned.shape[1], features)


LANES = 128
TILE = 8
STEPS = 2
WIDE = 512
RELAYED = ((0, 0), (1, 1), (2, 4), (5, 3), (4, 2), (3, 5), (6, 6), (7, 7))
VMEM = pl.BlockSpec(memory_space=pltpu.VMEM)
HBM = pl.BlockSpec(memory_space=pltpu.HBM)


class Plan:
    def __init__(self, rows, cols, rows_first, rows_second, features, channels):
        self.rows, self.cols = rows, cols
        self.rows_first, self.rows_second = rows_first, rows_second
        self.features, self.channels = features, channels
        self.length_first = rows_first * rows
        self.length_second = rows_second * cols
        self.positions = self.length_first * self.length_second
        self.groups = channels // GROUP
        self.full = self.groups // rows
        self.sub = GROUP // rows
        self.half = rows_second // 2
        self.quads = -(-self.half // rows)
        self.tiles = self.full * self.half + self.quads
        self.local = rows_first * rows_second
        self.half_wide = rows // 2 * self.full * GROUP
        self.send_rows = self.full * self.local + 2 * self.quads * TILE
        self.pairs = self.length_first // cols // 2
        self.block_b = self.length_second // rows
        self.out_rows = self.block_b * 2 * self.pairs
        self.row_tiles = self.out_rows // TILE
        self.back_quads = -(-self.row_tiles // rows)
        self.back_rows = self.full * self.out_rows + self.back_quads * TILE

    def fits(self):
        return (
            GROUP == LANES
            and self.rows & (self.rows - 1) == 0
            and self.cols & (self.cols - 1) == 0
            and 1 < self.rows <= 8
            and self.cols > 1
            and self.rows_first == TILE
            and self.rows_second % 2 == 0
            and self.channels % GROUP == 0
            and self.groups % self.rows == 1
            and self.full == 2
            and self.length_first == 4 * self.cols
            and self.length_second % self.rows == 0
            and 2 * self.block_b % TILE == 0
            and self.features % 512 == 0
        )


def channel_table():
    j = np.arange(GROUP)[:, None]
    u = np.arange(GROUP)[None, :]
    half = GROUP // 2
    m = np.where(u <= half, u, u - half)
    angle = 2.0 * np.pi * (j * m % GROUP) / GROUP
    return np.where(u <= half, np.cos(angle), np.sin(angle))


def unfold_table():
    half = GROUP // 2
    table = np.zeros((GROUP, GROUP))
    for m in range(GROUP):
        near = m if m <= half else GROUP - m
        table[near, m] = 1.0
        if 0 < near < half:
            table[half + near, m] = -1.0 if m < half else 1.0
    return table


def paired(table):
    zero = np.zeros_like(table)
    return np.block([[table, zero], [zero, table]])


def first_tables(plan):
    a = np.arange(plan.length_first)
    out = np.zeros((plan.cols, plan.half, plan.cols, plan.pairs, 2, 2, 2, plan.length_first))
    for col in range(plan.cols):
        for b9 in range(plan.half):
            for h in range(2):
                b = col * plan.rows_second + h * plan.half + b9
                for c in range(plan.cols):
                    for i in range(plan.pairs):
                        k = c * plan.pairs + i
                        if k == 0:
                            out[col, b9, c, i, h, 0, h] = 1.0
                            out[col, b9, c, i, h, 1, h] = np.where(a % 2 == 0, 1.0, -1.0)
                        else:
                            phase = (a * plan.length_second + b) * k % plan.positions
                            angle = 2.0 * np.pi * phase / plan.positions
                            out[col, b9, c, i, h, 0, h] = np.cos(angle)
                            out[col, b9, c, i, h, 1, h] = -np.sin(angle)
    size = 2 * plan.length_first
    return out.reshape(plan.cols, plan.half, size, size)


def second_tables(plan):
    length = plan.length_second
    b9 = np.arange(plan.half)[:, None, None]
    c = np.arange(plan.cols)[None, :, None]
    h = np.arange(2)[None, None, :]
    b = (c * plan.rows_second + h * plan.half + b9).reshape(-1)
    k = np.arange(length)
    angle = 2.0 * np.pi * (k[:, None] * b[None, :] % length) / length
    cos, sin = np.cos(angle), np.sin(angle)
    cosine = np.stack([cos, sin], axis=-1)
    sine = np.stack([sin, -cos], axis=-1)

    def arrange(plus, minus):
        both = np.stack([plus, minus]).reshape(2, plan.rows, plan.block_b, -1)
        return both.transpose(1, 0, 2, 3).reshape(2 * length, -1)

    usual = np.stack([arrange(cosine, cosine[::-1]), arrange(sine, -sine[::-1])])
    turn = 2.0 * np.pi * ((plan.length_first // 2) * b % plan.positions) / plan.positions
    late = angle + turn[None, :]
    zero = np.zeros_like(cos)
    first = np.stack(
        [
            arrange(np.stack([cos, zero], -1), np.stack([zero, np.cos(late)], -1)),
            arrange(np.stack([sin, zero], -1), np.stack([zero, np.sin(late)], -1)),
        ]
    )
    return usual, first


def order_table(plan):
    table = np.zeros((plan.out_rows, plan.out_rows))
    for i in range(plan.pairs):
        for neg in range(2):
            for k in range(plan.block_b):
                row = (k * 2 + neg) * plan.pairs + i
                table[row, (i * 2 + neg) * plan.block_b + k] = 1.0
    return table


def dot(left, right):
    return jnp.dot(left, right, preferred_element_type=jnp.float32)


def lane_index(shape):
    return lax.broadcasted_iota(jnp.int32, shape, 1)


def turn_lanes(value, amount):
    amount = amount % LANES
    return value if amount == 0 else pltpu.roll(value, amount, 1)


def by_lane(pieces, sub):
    out = pieces[0]
    lane = lane_index(out.shape)
    for n in range(1, len(pieces)):
        out = jnp.where(lane >= n * sub, pieces[n], out)
    return out


def far_kernel(
    plan, depth, x_hbm, gain_hbm, w_hbm, table_hbm, out_ref, near_ref, normed_ref, x_ref, gain_ref, table_ref, w_ref, sems, w_sems
):
    wide = plan.half_wide
    other = 1 - lax.axis_index("row") // (plan.rows // 2)
    x_copy = pltpu.make_async_copy(x_hbm, x_ref, sems.at[0])
    gain_copy = pltpu.make_async_copy(gain_hbm, gain_ref, sems.at[1])
    table_copy = pltpu.make_async_copy(table_hbm, table_ref, sems.at[2])
    x_copy.start()
    gain_copy.start()
    steps = plan.features // depth
    copies = []
    for n in range(steps):
        rows = pl.ds(n * depth, depth)
        far = pltpu.make_async_copy(
            w_hbm.at[rows, pl.ds(pl.multiple_of(other * wide, LANES), wide)],
            w_ref.at[rows, pl.ds(0, wide)],
            w_sems.at[0, n],
        )
        last = pltpu.make_async_copy(
            w_hbm.at[rows, pl.ds(2 * wide, GROUP)], w_ref.at[rows, pl.ds(wide, GROUP)], w_sems.at[1, n]
        )
        far.start()
        last.start()
        copies.append((far, last))
    table_copy.start()
    gain_copy.wait()
    gain = gain_ref[...].astype(jnp.float32)
    x_copy.wait()
    step = 48 if plan.local % 48 == 0 else TILE
    for start in range(0, plan.local, step):
        rows = slice(start, start + step)
        total = jnp.zeros((step, LANES), jnp.float32)
        for n in range(plan.features // LANES):
            part = x_ref[rows, n * LANES : (n + 1) * LANES].astype(jnp.float32)
            total = total + part * part
        mean = jnp.sum(total, axis=-1, keepdims=True) * (1.0 / plan.features)
        scale = lax.rsqrt(mean + norm_eps)
        for n in range(plan.features // LANES):
            columns = slice(n * LANES, (n + 1) * LANES)
            part = x_ref[rows, columns].astype(jnp.float32)
            normed_ref[rows, columns] = (part * scale * gain[n : n + 1, :]).astype(jnp.bfloat16)
    total = None
    for n in range(steps):
        for copy in copies[n]:
            copy.wait()
        rows = slice(n * depth, (n + 1) * depth)
        part = dot(normed_ref[:, rows], w_ref[rows, :])
        total = part if n == 0 else total + part
    mapped = total.astype(jnp.bfloat16)
    table_copy.wait()
    values = dot(mapped[:, wide:], table_ref[:GROUP, :GROUP])
    sub, base = plan.sub, plan.full * plan.local
    turned = [turn_lanes(values, sub * t).astype(jnp.bfloat16) for t in range(plan.rows)]
    lower = other == 0
    for dest in range(plan.rows // 2):
        for h in range(2):
            for quad in range(plan.quads):
                ends = []
                for high in range(2):
                    pieces = []
                    for inner in range(plan.rows):
                        b9 = quad * plan.rows + inner
                        if b9 < plan.half:
                            row = (h * plan.half + b9) * TILE
                            turn = (inner - dest - high * (plan.rows // 2)) % plan.rows
                            pieces.append(turned[turn][row : row + TILE, :])
                    ends.append(by_lane(pieces, sub))
                at = (h * plan.quads + quad) * TILE
                out_ref[dest, base + at : base + at + TILE, :] = jnp.where(lower, ends[0], ends[1])
                near_ref[dest, at : at + TILE, :] = jnp.where(lower, ends[1], ends[0])
    spread(plan, mapped, table_ref, out_ref)


def spread(plan, mapped, table_ref, out_ref):
    for dest in range(plan.rows // 2):
        values = dot(mapped[:, dest * 2 * GROUP : (dest + 1) * 2 * GROUP], table_ref[...])
        for f in range(plan.full):
            out_ref[dest, f * plan.local : (f + 1) * plan.local, :] = values[
                :, f * GROUP : (f + 1) * GROUP
            ].astype(jnp.bfloat16)


def near_kernel(plan, depth, normed_ref, near_ref, w_hbm, table_hbm, out_ref, table_ref, w_ref, sem, w_sems):
    wide = plan.half_wide
    mine = lax.axis_index("row") // (plan.rows // 2)
    steps = plan.features // depth
    copies = []
    for n in range(steps):
        rows = pl.ds(n * depth, depth)
        copy = pltpu.make_async_copy(
            w_hbm.at[rows, pl.ds(pl.multiple_of(mine * wide, LANES), wide)], w_ref.at[rows, :], w_sems.at[n]
        )
        copy.start()
        copies.append(copy)
    table_copy = pltpu.make_async_copy(table_hbm, table_ref, sem)
    table_copy.start()
    out_ref[:, plan.full * plan.local :, :] = near_ref[...]
    total = None
    for n in range(steps):
        copies[n].wait()
        rows = slice(n * depth, (n + 1) * depth)
        part = dot(normed_ref[:, rows], w_ref[rows, :])
        total = part if n == 0 else total + part
    table_copy.wait()
    spread(plan, total.astype(jnp.bfloat16), table_ref, out_ref)


def first_kernel(plan, *refs):
    slabs, (table_ref, out_ref, held_ref) = refs[: plan.rows], refs[plan.rows :]
    row = lax.axis_index("row")
    for s in range(plan.rows):
        held_ref[row ^ s] = slabs[s][...]
    for b9 in range(plan.half):
        quad, inner = divmod(b9, plan.rows)
        columns = []
        for f in range(plan.full):
            parts = []
            for h in range(2):
                at = f * plan.local + (h * plan.half + b9) * TILE
                parts += [held_ref[r, at : at + TILE, :] for r in range(plan.rows)]
            columns.append(jnp.concatenate(parts, axis=0))
        parts = []
        for h in range(2):
            at = plan.full * plan.local + (h * plan.quads + quad) * TILE
            parts += [held_ref[r, at : at + TILE, :] for r in range(plan.rows)]
        columns.append(jnp.concatenate(parts, axis=0))
        result = dot(table_ref[b9], jnp.concatenate(columns, axis=1))
        for f in range(plan.full):
            at = (f * plan.half + b9) * TILE
            piece = result[:, f * LANES : (f + 1) * LANES].astype(jnp.bfloat16)
            for c in range(plan.cols):
                out_ref[c, at : at + TILE, :] = piece[c * TILE : (c + 1) * TILE, :]
        tail = result[:, plan.full * LANES :]
        packed = tail if inner == 0 else jnp.where(lane_index(tail.shape) >= inner * plan.sub, tail, packed)
        if inner == plan.rows - 1 or b9 == plan.half - 1:
            at = (plan.full * plan.half + quad) * TILE
            piece = packed.astype(jnp.bfloat16)
            for c in range(plan.cols):
                out_ref[c, at : at + TILE, :] = piece[c * TILE : (c + 1) * TILE, :]


def second_far_kernel(plan, scaling, *refs):
    slabs = refs[: plan.cols]
    usual_ref, first_ref, out_ref, rhs_ref, held_ref = refs[plan.cols :]
    col = lax.axis_index("col")
    for s, pair in enumerate(crossing(plan.cols)):
        held_ref[col ^ by_parity(col, pair)] = slabs[s][: plan.tiles * TILE, :]
    sub, quarter = plan.sub, TILE // 2
    low = lax.broadcasted_iota(jnp.int32, (TILE, LANES), 0) < quarter
    for b9 in range(plan.half):
        quad, inner = divmod(b9, plan.rows)
        places = [(f * plan.half + b9) * TILE for f in range(plan.full)]
        places.append((plan.full * plan.half + quad) * TILE)
        for p in range(plan.cols // 2):
            at = b9 * (plan.cols // 2) * TILE + p * TILE
            for n, place in enumerate(places):
                even = held_ref[2 * p, place : place + TILE, :].astype(jnp.float32)
                odd = held_ref[2 * p + 1, place : place + TILE, :].astype(jnp.float32)
                both = [
                    jnp.where(low, even, pltpu.roll(odd, quarter, 0)),
                    jnp.where(low, pltpu.roll(even, quarter, 0), odd),
                ]
                for i in range(plan.pairs):
                    value = both[i]
                    if n == plan.full:
                        value = turn_lanes(value, -inner * sub)
                    rhs_ref[i, at : at + TILE, n * LANES : (n + 1) * LANES] = value.astype(jnp.bfloat16)
    other = 1 - lax.axis_index("row") // (plan.rows // 2)
    transform(plan, scaling, other, usual_ref, first_ref, rhs_ref, out_ref)


def second_near_kernel(plan, scaling, usual_ref, first_ref, rhs_ref, out_ref):
    mine = lax.axis_index("row") // (plan.rows // 2)
    transform(plan, scaling, mine, usual_ref, first_ref, rhs_ref, out_ref)


def transform(plan, scaling, which, usual_ref, first_ref, rhs_ref, out_ref):
    row = lax.axis_index("row")
    sub = plan.sub
    wide = (plan.full + 1) * LANES
    lane = lane_index((1, wide))
    last = lane >= plan.full * LANES
    place = jnp.where(last, lane - plan.full * LANES + row * sub, lane & (LANES - 1))
    is_sine = place > GROUP // 2
    span = 2 * plan.block_b
    devices = plan.rows // 2
    size, total = devices * span, plan.rows * span
    tails = {}
    for i in range(plan.pairs):
        table = first_ref if i == 0 else usual_ref
        start = pl.multiple_of(which * size, TILE)
        rows = jnp.concatenate([table[pl.ds(start, size), :], table[pl.ds(total + start, size), :]], axis=0)
        both = dot(rows, rhs_ref[i])
        for r in range(devices):
            cosine, sine = both[r * span : (r + 1) * span, :], both[size + r * span : size + (r + 1) * span, :]
            merged = jnp.where(is_sine, sine, cosine) * scaling
            for f in range(plan.full):
                at = f * plan.out_rows + i * span
                out_ref[r, at : at + span, :] = merged[:, f * LANES : (f + 1) * LANES].astype(jnp.bfloat16)
            tails[i, r] = merged[:, plan.full * LANES :]
    for r in range(devices):
        pieces = []
        for t in range(plan.row_tiles):
            i, at = divmod(t * TILE, span)
            pieces.append(turn_lanes(tails[i, r][at : at + TILE, :], (t % plan.rows) * sub))
        for whole in range(plan.back_quads):
            at = plan.full * plan.out_rows + whole * TILE
            group = pieces[whole * plan.rows : (whole + 1) * plan.rows]
            out_ref[r, at : at + TILE, :] = by_lane(group, sub).astype(jnp.bfloat16)


def unfolded(plan, order, unfold, slabs):
    pair = [slabs[f * plan.out_rows : (f + 1) * plan.out_rows, :] for f in range(plan.full)]
    ordered = dot(order, jnp.concatenate(pair, axis=1)).astype(jnp.bfloat16)
    return dot(ordered, unfold).astype(jnp.bfloat16)


def arrivals(rows):
    return [rows - 1, *range(1, rows - 1)]


def early_kernel(plan, slab_ref, unfold_ref, order_ref, w_hbm, partial_ref, w_ref, own_ref, raw_ref, sems):
    row = lax.axis_index("row")
    each = plan.full * GROUP

    def part(s):
        return w_hbm.at[pl.ds(pl.multiple_of((row ^ s) * each, LANES), each), :]

    copies = [pltpu.make_async_copy(part(0), own_ref, sems.at[0])]
    for n, s in enumerate(arrivals(plan.rows)):
        copies.append(pltpu.make_async_copy(part(s), raw_ref.at[pl.ds(n * each, each), :], sems.at[s]))
    copies.append(
        pltpu.make_async_copy(
            w_hbm.at[pl.ds(plan.rows * each, GROUP), :],
            raw_ref.at[pl.ds((plan.rows - 1) * each, GROUP), :],
            sems.at[plan.rows],
        )
    )
    for copy in copies:
        copy.start()
    unfold = unfold_ref[...]
    spectrum = unfolded(plan, order_ref[...], unfold, slab_ref)
    copies[0].wait()
    for n in range(plan.features // WIDE):
        columns = slice(n * WIDE, (n + 1) * WIDE)
        partial_ref[:, columns] = dot(spectrum, own_ref[:, columns])
    for s in range(1, plan.rows + 1):
        copies[s].wait()
        size = each if s < plan.rows else GROUP
        rows = slice((s - 1) * each, (s - 1) * each + size)
        for n in range(plan.features // 512):
            columns = slice(n * 512, (n + 1) * 512)
            w_ref[rows, columns] = dot(unfold[:size, :size], raw_ref[rows, columns]).astype(jnp.bfloat16)


def middle_kernel(plan, slab_ref, order_ref, w_ref, partial_ref, out_ref):
    pair = [slab_ref[f * plan.out_rows : (f + 1) * plan.out_rows, :] for f in range(plan.full)]
    ordered = dot(order_ref[...], jnp.concatenate(pair, axis=1)).astype(jnp.bfloat16)
    for n in range(plan.features // 512):
        columns = slice(n * 512, (n + 1) * 512)
        out_ref[:, columns] = partial_ref[:, columns] + dot(ordered, w_ref[: plan.full * GROUP, columns])


def tail_kernel(plan, *refs):
    slabs = refs[: plan.rows]
    order_ref, partial_ref, w_ref, out_hbm, packed_ref, stage_ref, sems = refs[plan.rows :]
    row = lax.axis_index("row")
    main = plan.full * plan.out_rows
    for s in range(plan.rows):
        packed_ref[row ^ s] = slabs[s][main:, :]
    packed = [packed_ref[q].astype(jnp.float32) for q in range(plan.rows)]
    turned = [[turn_lanes(value, plan.sub * t) for t in range(plan.rows)] for value in packed]
    pieces = []
    for t in range(plan.row_tiles):
        whole, inner = divmod(t, plan.rows)
        rows = slice(whole * TILE, (whole + 1) * TILE)
        pieces.append(
            by_lane([turned[q][(q - inner) % plan.rows][rows, :] for q in range(plan.rows)], plan.sub)
        )
    parts = []
    for s in arrivals(plan.rows)[1:]:
        parts += [slabs[s][f * plan.out_rows : (f + 1) * plan.out_rows, :] for f in range(plan.full)]
    parts.append(jnp.concatenate(pieces, axis=0).astype(jnp.bfloat16))
    ordered = dot(order_ref[...], jnp.concatenate(parts, axis=1)).astype(jnp.bfloat16)
    group = 2 * plan.pairs
    copies = []
    for n in range(plan.features // WIDE):
        columns = slice(n * WIDE, (n + 1) * WIDE)
        result = (partial_ref[:, columns] + dot(ordered, w_ref[plan.full * GROUP :, columns])).astype(jnp.bfloat16)
        for k in range(plan.block_b):
            stage_ref[n, k] = result[k * group : (k + 1) * group, :]
        copy = pltpu.make_async_copy(stage_ref.at[n], out_hbm.at[:, :, pl.ds(n * WIDE, WIDE)], sems.at[n])
        copy.start()
        copies.append(copy)
    for copy in copies:
        copy.wait()


def estimate(flops, moved):
    return pl.CostEstimate(flops=flops, bytes_accessed=moved, transcendentals=0)


def limit(mebibytes):
    return pltpu.CompilerParams(vmem_limit_bytes=mebibytes * 2**20)


def by_parity(index, pair):
    return pair[0] + (index % 2) * (pair[1] - pair[0])


def exchange(values, axis, size):
    here = lax.axis_index(axis)
    out = []
    for s in range(size):
        there = here ^ s
        if isinstance(values, tuple):
            source, index = values[2 * s // size], there % (size // 2)
        else:
            source, index = values, there
        slab = lax.dynamic_index_in_dim(source, index, 0, keepdims=False)
        if s:
            slab = lax.ppermute(slab, axis, [(n, n ^ s) for n in range(size)])
        out.append(slab)
    return out


def crossing(cols):
    if cols == len(RELAYED):
        return RELAYED
    return tuple((s, s) for s in range(cols))


def cross(values, cols):
    if cols != len(RELAYED):
        return exchange(values, "col", cols)
    here = lax.axis_index("col")

    def slab(pair, flip=0):
        return lax.dynamic_index_in_dim(values, here ^ by_parity(here, pair) ^ flip, 0, keepdims=False)

    def send(value, pair):
        return lax.ppermute(value, "col", [(n, n ^ pair[n % 2]) for n in range(cols)])

    def both(pair):
        return jnp.concatenate([slab(pair), slab(pair, 1)], axis=0)

    rows = values.shape[1]
    diagonal = send(both((6, 6)), (6, 6))
    beside = send(both((4, 2)), (4, 2))
    crossed = send(slab((3, 5)), (3, 5))
    straight = send(slab((2, 4)), (2, 4))
    sibling = send(slab((1, 1)), (1, 1))
    diagonal_other = send(diagonal[rows:], (1, 1))
    beside_other = send(beside[rows:], (1, 1))
    return [slab((0, 0)), sibling, straight, crossed, beside, beside_other, diagonal, diagonal_other]


def packed(plan, tokens, norm_gain, w_in, w_out):
    half_type = jnp.bfloat16
    scaling = 1.0 / math.sqrt(plan.positions * GROUP)
    col = lax.axis_index("col")
    local, features, channels = plan.local, plan.features, plan.channels
    x = tokens.transpose(1, 0, 2).reshape(local, features)
    channel = jnp.asarray(paired(channel_table()), half_type)
    gain = norm_gain.reshape(features // LANES, LANES)
    x, gain, w_in, channel = (pltpu.with_memory_space_constraint(v, pltpu.HBM) for v in (x, gain, w_in, channel))
    depth, wide = features // STEPS, plan.half_wide
    packed_rows = 2 * plan.quads * TILE
    far, near, normed = pl.pallas_call(
        functools.partial(far_kernel, plan, depth),
        out_shape=(
            pltpu.VMEM((plan.rows // 2, plan.send_rows, LANES), half_type),
            pltpu.VMEM((plan.rows // 2, packed_rows, LANES), half_type),
            pltpu.VMEM((local, features), half_type),
        ),
        in_specs=[HBM] * 4,
        out_specs=(VMEM, VMEM, VMEM),
        scratch_shapes=[
            pltpu.VMEM((local, features), half_type),
            pltpu.VMEM((features // LANES, LANES), half_type),
            pltpu.VMEM((2 * GROUP, 2 * GROUP), half_type),
            pltpu.VMEM((features, wide + GROUP), half_type),
            pltpu.SemaphoreType.DMA((3,)),
            pltpu.SemaphoreType.DMA((2, STEPS)),
        ],
        compiler_params=pltpu.CompilerParams(vmem_limit_bytes=16 * 2**20),
        cost_estimate=estimate(local * features * channels, features * channels),
        name="far",
    )(x, gain, w_in, channel)
    close = pl.pallas_call(
        functools.partial(near_kernel, plan, depth),
        out_shape=pltpu.VMEM((plan.rows // 2, plan.send_rows, LANES), half_type),
        in_specs=[VMEM, VMEM, HBM, HBM],
        out_specs=VMEM,
        scratch_shapes=[
            pltpu.VMEM((2 * GROUP, 2 * GROUP), half_type),
            pltpu.VMEM((features, wide), half_type),
            pltpu.SemaphoreType.DMA,
            pltpu.SemaphoreType.DMA((STEPS,)),
        ],
        compiler_params=pltpu.CompilerParams(vmem_limit_bytes=8 * 2**20),
        cost_estimate=estimate(local * features * channels, features * channels),
        name="near",
    )(normed, near, w_in, channel)
    slabs = exchange((close, far), "row", plan.rows)
    first = lax.dynamic_index_in_dim(jnp.asarray(first_tables(plan), half_type), col, 0, keepdims=False)
    turned = pl.pallas_call(
        functools.partial(first_kernel, plan),
        out_shape=jax.ShapeDtypeStruct((plan.cols, plan.tiles * TILE, LANES), half_type),
        in_specs=[VMEM] * (plan.rows + 1),
        out_specs=VMEM,
        scratch_shapes=[pltpu.VMEM((plan.rows, plan.send_rows, LANES), half_type)],
        compiler_params=limit(8),
        cost_estimate=estimate(10**8, 10**6),
        name="first",
    )(*slabs, first)
    slabs = cross(turned, plan.cols)
    usual, special = (jnp.asarray(table, half_type) for table in second_tables(plan))
    usual, special = (table.reshape(-1, table.shape[-1]) for table in (usual, special))
    leading = jnp.where(col == 0, special, usual)
    depth = plan.half * plan.cols * 4
    slab = pltpu.VMEM((plan.rows // 2, plan.back_rows, LANES), half_type)
    rhs = pltpu.VMEM((plan.pairs, depth, (plan.full + 1) * LANES), half_type)
    back_far, rhs = pl.pallas_call(
        functools.partial(second_far_kernel, plan, scaling),
        out_shape=(slab, rhs),
        in_specs=[VMEM] * (plan.cols + 2),
        out_specs=(VMEM, VMEM),
        scratch_shapes=[pltpu.VMEM((plan.cols, plan.tiles * TILE, LANES), half_type)],
        compiler_params=limit(12),
        cost_estimate=estimate(3 * 10**8, 10**6),
        name="second_far",
    )(*slabs, usual, leading)
    back_near = pl.pallas_call(
        functools.partial(second_near_kernel, plan, scaling),
        out_shape=slab,
        in_specs=[VMEM] * 3,
        out_specs=VMEM,
        compiler_params=limit(12),
        cost_estimate=estimate(3 * 10**8, 10**6),
        name="second_near",
    )(usual, leading, rhs)
    slabs = exchange((back_near, back_far), "row", plan.rows)
    unfold = jnp.asarray(paired(unfold_table()), half_type)
    order = jnp.asarray(order_table(plan), half_type)
    main, each = plan.full * plan.out_rows, plan.full * GROUP
    cost = estimate(local * features * channels, features * channels)
    partial, w_rest = pl.pallas_call(
        functools.partial(early_kernel, plan),
        out_shape=(
            pltpu.VMEM((plan.out_rows, features), jnp.float32),
            pltpu.VMEM((channels - each, features), half_type),
        ),
        in_specs=[VMEM] * 3 + [HBM],
        out_specs=(VMEM, VMEM),
        scratch_shapes=[
            pltpu.VMEM((each, features), half_type),
            pltpu.VMEM((channels - each, features), half_type),
            pltpu.SemaphoreType.DMA((plan.rows + 1,)),
        ],
        compiler_params=limit(14),
        cost_estimate=cost,
        name="early",
    )(slabs[0], unfold, order, pltpu.with_memory_space_constraint(w_out, pltpu.HBM))
    partial = pl.pallas_call(
        functools.partial(middle_kernel, plan),
        out_shape=pltpu.VMEM((plan.out_rows, features), jnp.float32),
        in_specs=[VMEM] * 4,
        out_specs=VMEM,
        compiler_params=limit(8),
        cost_estimate=estimate(10**8, 10**6),
        name="middle",
    )(slabs[plan.rows - 1], order, w_rest, partial)
    return pl.pallas_call(
        functools.partial(tail_kernel, plan),
        out_shape=jax.ShapeDtypeStruct((plan.block_b, 2 * plan.pairs, features), half_type),
        in_specs=[VMEM] * (plan.rows + 3),
        out_specs=HBM,
        scratch_shapes=[
            pltpu.VMEM((plan.rows, plan.back_rows - main, LANES), half_type),
            pltpu.VMEM((features // WIDE, plan.block_b, 2 * plan.pairs, WIDE), half_type),
            pltpu.SemaphoreType.DMA((features // WIDE,)),
        ],
        compiler_params=limit(12),
        cost_estimate=cost,
        name="tail",
    )(*slabs, order, partial, w_rest)


def shards(tokens, norm_gain, w_in, w_out):
    rows_first, rows_second, features = tokens.shape
    plan = Plan(
        lax.axis_size("row"), lax.axis_size("col"), rows_first, rows_second, features, w_in.shape[1]
    )
    if plan.fits():
        return packed(plan, tokens, norm_gain, w_in, w_out)
    return general(tokens, norm_gain, w_in, w_out)


def solution(mesh):
    in_specs = (P("row", "col", None), P(), P(), P())
    out_specs = P("row", "col", None)

    return jax.shard_map(shards, mesh=mesh, in_specs=in_specs, out_specs=out_specs, check_vma=False)
```
